1024 devices in a mesh: kv: 128 (over z, y), tp: 8 (over x, core).
Axes of the slice: x: 4, y: 4, z: 32, core: 2. Of those that a mesh axis runs over, the one named last changes fastest.
Arguments:
- tokens: bfloat16 [32768, 2048], P('kv'), may hold values from -6 to 6
- query_weight: bfloat16 [2048, 2048], P(None, 'tp'), may hold values from -0.125 to 0.125
- key_weight: bfloat16 [2048, 512], P(None, 'tp'), may hold values from -0.125 to 0.125
- value_weight: bfloat16 [2048, 512], P(None, 'tp'), may hold values from -0.125 to 0.125
- gate_weight: bfloat16 [2048, 64], replicated, may hold values from -0.125 to 0.125
- query_gain: float32 [64], replicated
- key_gain: float32 [64], replicated
- out_weight: bfloat16 [2048, 2048], P('tp'), may hold values from -0.125 to 0.125
- shared_block: int32 [128], P('kv'), may hold values from 0 to 3, as said below
- chosen_device: int32 [512, 15], P('kv'), may hold values from 0 to 127, as said below
Outputs:
- mixed_out: bfloat16 [32768, 2048], P(('kv', 'tp'))
- log_weight: float32 [2, 32768, 32], P(None, 'kv', 'tp')
The draws below stay inside these ranges and needn't reach their ends.
Inputs may be any that keep to these rules, and one draw needn't show every extreme that they name: `shared_block`: entry d names one of the 64-position blocks of device d's 256 positions. `chosen_device`: row b names 15 different devices, never the device that holds query block b.
All inputs are finite; a program needn't handle non-finite values.
Results may differ from the reference program's by a relative error of at most 0.019.
The reference program's roundings to bfloat16 on the way count: a program that leaves them out, or rounds other values in their place, can miss the bound.
Values may be sent and summed in bfloat16 or wider, within the bound.
No kernel may reach another device: no remote copies, remote signals or barrier semaphores. Data moves between devices by JAX's collectives and lax.ppermute only.
A program may use at most 32 MiB of HBM per device.

```python
import jax
import jax.numpy as jnp
from jax import lax

D = 2048
H = 32
HD = 64
G = 8
TOK_DEV = 256
SEL = 64
CMP = 32
NREM = 15
SEQ = 32768
NQB = 512
N_KV = 128
N_TP = 8


def plan_blocks(key):
    per_device = TOK_DEV // SEL
    shared_numbers = jax.random.randint(jax.random.fold_in(key, 11), (N_KV,), 0, per_device)
    owning_devices = jnp.arange(N_KV, dtype=jnp.int32)
    home_device = jnp.arange(NQB, dtype=jnp.int32) // per_device
    frequent_blocks = jax.random.randint(jax.random.fold_in(key, 12), (N_KV,), 0, 4) == 0
    added_reward = jnp.where(frequent_blocks, 2048, 0)
    noise_values = jax.random.randint(jax.random.fold_in(key, 13), (NQB, N_KV), 0, 2048)
    forced = (owning_devices[None, :] == home_device[:, None] - 1) | (owning_devices[None, :] == home_device[:, None] - N_KV // 2) & (home_device[:, None] >= N_KV // 2)
    earlier = owning_devices[None, :] < home_device[:, None]
    block_priority = jnp.where(owning_devices[None, :] == home_device[:, None], 0, jnp.where(forced, 3, jnp.where(earlier, 2, 1)))
    block_ranking = (block_priority * 4096 + added_reward[None, :] + noise_values) * N_KV + owning_devices[None, :]
    ignored, selected = lax.top_k(block_ranking, NREM)
    return (shared_numbers.astype(jnp.int32), selected.astype(jnp.int32))


def draw_shared_block(key, part):
    return plan_blocks(key)[0]


def draw_chosen_device(key, part):
    return plan_blocks(key)[1]


def draw_query_gain(key, part):
    return jax.random.uniform(jax.random.fold_in(key, 21), (HD,), jnp.float32, 0.6, 1.6)


def draw_key_gain(key, part):
    return jax.random.uniform(jax.random.fold_in(key, 22), (HD,), jnp.float32, 0.6, 1.6)


def level_of(rng, shape, cuts, least, largest):
    def one(dim, shards_of):
        heights = jax.random.uniform(jax.random.fold_in(jax.random.fold_in(rng, 6), dim), (shards_of,), jnp.float32, least / len(cuts), largest / len(cuts))
        return jnp.repeat(jnp.exp(heights), shape[dim] // shards_of).reshape((-1,) + (1,) * (len(shape) - dim - 1))

    level = one(*cuts[0])
    for cut in cuts[1:]:
        level = level * one(*cut)
    return level


def centred(rng, dims, width, bound, shards=(), kind=jnp.bfloat16):
    array = jax.random.normal(rng, dims, jnp.float32) * width
    if len(shards) > 0:
        array = level_of(rng, dims, shards, -0.22, 0.18) * array
    return jnp.clip(array, min=-bound, max=bound).astype(kind)


def setup_inputs(seed: int = 0) -> dict:
    seeds = jax.random.split(jax.random.key(seed), 11)
    tokens = centred(seeds[0], (SEQ, D), 1.0, 6.0, ((0, 128),))
    query_weight = centred(seeds[1], (D, H * HD), D ** -0.5, 0.125, ((1, 8),))
    key_weight = centred(seeds[2], (D, G * HD), D ** -0.5, 0.125, ((1, 8),))
    value_weight = centred(seeds[3], (D, G * HD), D ** -0.5, 0.125, ((1, 8),))
    gate_weight = centred(seeds[4], (D, 2 * H), D ** -0.5, 0.125)
    query_gain = draw_query_gain(jax.random.fold_in(seeds[10], 71), 0)
    key_gain = draw_key_gain(jax.random.fold_in(seeds[10], 71), 0)
    out_weight = centred(seeds[7], (H * HD, D), (H * HD) ** -0.5, 0.125, ((0, 8),))
    shared_block = draw_shared_block(jax.random.fold_in(seeds[10], 71), 0)
    chosen_device = draw_chosen_device(jax.random.fold_in(seeds[10], 71), 0)
    return {"tokens": tokens, "query_weight": query_weight, "key_weight": key_weight, "value_weight": value_weight, "gate_weight": gate_weight, "query_gain": query_gain, "key_gain": key_gain, "out_weight": out_weight, "shared_block": shared_block, "chosen_device": chosen_device}


norm_eps = 1e-06
rope_base = 500000.0
big_negative = -1e+30

def rounded(values_in):
    return lax.optimization_barrier(values_in.astype(jnp.bfloat16))

def unit_norm(values_in, gain_vec):
    upcast = values_in.astype(jnp.float32)
    return upcast * lax.rsqrt(lax.optimization_barrier(jnp.mean(upcast * upcast, axis=-1, keepdims=True)) + norm_eps) * gain_vec

def rotate(values_in, places):
    half_size = values_in.shape[-1] // 2
    inverse = jnp.power(rope_base, -jnp.arange(half_size, dtype=jnp.float32) * 2.0 / values_in.shape[-1])
    angles = places.astype(jnp.float32)[:, None] * inverse[None, :]
    cos_vals = jnp.cos(angles)[:, None, :]
    sin_vals = jnp.sin(angles)[:, None, :]
    upcast = values_in.astype(jnp.float32)
    front_half = upcast[..., :half_size]
    back_half = upcast[..., half_size:]
    return jnp.concatenate([front_half * cos_vals - back_half * sin_vals, back_half * cos_vals + front_half * sin_vals], axis=-1)

def reference(tokens, query_weight, key_weight, value_weight, gate_weight, query_gain, key_gain, out_weight, shared_block, chosen_device):
    seq_len = tokens.shape[0]
    per_group = H // G
    places = jnp.arange(seq_len, dtype=jnp.int32)
    queries = rounded(jnp.dot(tokens, query_weight, preferred_element_type=jnp.float32)).reshape(seq_len, H, HD)
    keys_raw = rounded(jnp.dot(tokens, key_weight, preferred_element_type=jnp.float32)).reshape(seq_len, G, HD)
    values_raw = rounded(jnp.dot(tokens, value_weight, preferred_element_type=jnp.float32)).reshape(seq_len, G, HD)
    q_plain = rounded(unit_norm(queries, query_gain))
    k_plain = rounded(unit_norm(keys_raw, key_gain))
    q_turned = rounded(rotate(q_plain, places))
    k_turned = rounded(rotate(k_plain, places))
    gate_vals = jax.nn.sigmoid(jnp.dot(tokens, gate_weight, preferred_element_type=jnp.float32)).reshape(seq_len, H, 2)
    span_count = seq_len // CMP
    span_keys = rounded(lax.optimization_barrier(jnp.mean(k_plain.astype(jnp.float32).reshape(span_count, CMP, G, HD), axis=1))).astype(jnp.float32)
    span_values = rounded(lax.optimization_barrier(jnp.mean(values_raw.astype(jnp.float32).reshape(span_count, CMP, G, HD), axis=1))).astype(jnp.float32)
    span_ends = jnp.arange(span_count, dtype=jnp.int32) * CMP + CMP - 1
    blocks_dev = TOK_DEV // SEL
    block_numbers = (chosen_device * blocks_dev + shared_block[chosen_device]).astype(jnp.int32)
    key_blocks = k_turned.reshape(NQB, SEL, G, HD)
    value_blocks = values_raw.reshape(NQB, SEL, G, HD)
    score_scale = HD ** (-0.5)
    causal_own = jnp.arange(SEL)[None, :] <= jnp.arange(SEL)[:, None]

    def one_block(inputs):
        q_plain_b, q_turned_b, named_blocks, devices_named, block_num = inputs
        qplaces = block_num * SEL + jnp.arange(SEL, dtype=jnp.int32)
        scores = jnp.einsum('qghd,cgd->qghc', q_plain_b.astype(jnp.float32), span_keys) * score_scale
        allowed = (span_ends[None, :] <= qplaces[:, None])[:, None, None, :]
        has_span = (qplaces >= CMP - 1)[:, None, None]
        peak_val = lax.optimization_barrier(jnp.max(jnp.where(allowed, scores, big_negative), axis=-1))
        weights_raw = jnp.where(allowed, jnp.exp(scores - peak_val[..., None]), 0.0)
        divisor = jnp.where(has_span, lax.optimization_barrier(jnp.sum(weights_raw, axis=-1)), 1.0)
        span_out = jnp.einsum('qghc,cgd->qghd', rounded(weights_raw).astype(jnp.float32), span_values) / divisor[..., None]
        span_lse = jnp.where(has_span, peak_val + jnp.log(divisor), 0.0)
        key_rows = jnp.concatenate([key_blocks[block_num][None], key_blocks[named_blocks]], axis=0).reshape(-1, G, HD).astype(jnp.float32)
        value_rows = jnp.concatenate([value_blocks[block_num][None], value_blocks[named_blocks]], axis=0).reshape(-1, G, HD).astype(jnp.float32)
        remote_ok = jnp.repeat(devices_named < block_num // blocks_dev, SEL)
        allowed_sel = jnp.concatenate([causal_own, jnp.broadcast_to(remote_ok[None, :], (SEL, remote_ok.shape[0]))], axis=1)[:, None, None, :]
        scores_sel = jnp.einsum('qghd,kgd->qghk', q_turned_b.astype(jnp.float32), key_rows) * score_scale
        peak_sel = lax.optimization_barrier(jnp.max(jnp.where(allowed_sel, scores_sel, big_negative), axis=-1))
        weights_sel = jnp.where(allowed_sel, jnp.exp(scores_sel - peak_sel[..., None]), 0.0)
        sum_sel = lax.optimization_barrier(jnp.sum(weights_sel, axis=-1))
        chosen_out = jnp.einsum('qghk,kgd->qghd', rounded(weights_sel).astype(jnp.float32), value_rows) / sum_sel[..., None]
        return (span_out, chosen_out, span_lse, peak_sel + jnp.log(sum_sel))
    span_out, chosen_out, span_lse, chosen_lse = lax.map(one_block, (q_plain.reshape(NQB, SEL, G, per_group, HD), q_turned.reshape(NQB, SEL, G, per_group, HD), block_numbers, chosen_device, jnp.arange(NQB, dtype=jnp.int32)))
    span_out = span_out.reshape(seq_len, H, HD)
    chosen_out = chosen_out.reshape(seq_len, H, HD)
    mixed_heads = rounded(gate_vals[..., 0:1] * span_out + gate_vals[..., 1:2] * chosen_out).reshape(seq_len, H * HD)
    group_width = H * HD // N_TP
    accum_sum = jnp.zeros((seq_len, D), jnp.float32)
    for group_num in range(N_TP):
        partial_value = jnp.dot(mixed_heads[:, group_num * group_width:(group_num + 1) * group_width], out_weight[group_num * group_width:(group_num + 1) * group_width], preferred_element_type=jnp.float32)
        accum_sum = accum_sum + rounded(partial_value).astype(jnp.float32)
    mixed_out = accum_sum.astype(jnp.bfloat16)
    log_weight = jnp.stack([span_lse.reshape(seq_len, H), chosen_lse.reshape(seq_len, H)])
    return (mixed_out, log_weight)
```

```python
import jax
import jax.numpy as jnp
from jax import lax
from jax.sharding import Mesh
from jax.sharding import PartitionSpec as P

SEL = 64
CMP = 32
KV = ("z_far", "z_near", "y")
KV_TP = ("z_far", "z_near", "y", "tp")


norm_eps = 1e-06
rope_base = 500000.0
big_negative = -1e30


def spread(block, axis):
    count = lax.axis_size(axis)
    copies = lax.optimization_barrier(jnp.broadcast_to(block[None], (count, *block.shape)))
    return lax.all_to_all(copies, axis, split_axis=0, concat_axis=0, tiled=True)


def split_up(array, dim, length):
    lengths = array.shape
    pieces = array.reshape(*lengths[:dim], length, lengths[dim] // length, *lengths[dim + 1 :])
    return jnp.moveaxis(pieces, dim, 0)


def sent_and_summed(array, axis, dim):
    pieces = split_up(array, dim, lax.axis_size(axis))
    arrived = lax.all_to_all(pieces, axis, split_axis=0, concat_axis=0, tiled=True)
    return arrived.astype(jnp.float32).sum(axis=0)


def rounded(values_in):
    return lax.optimization_barrier(values_in.astype(jnp.bfloat16))


def unit_norm(values_in, gain_vec):
    upcast = values_in.astype(jnp.float32)
    return (
        upcast * lax.rsqrt(jnp.mean(upcast * upcast, axis=-1, keepdims=True) + norm_eps) * gain_vec
    )


def rotate(values_in, places):
    half_size = values_in.shape[-1] // 2
    inverse = jnp.power(
        rope_base, -jnp.arange(half_size, dtype=jnp.float32) * 2.0 / values_in.shape[-1]
    )
    angles = places.astype(jnp.float32)[:, None] * inverse[None, :]
    cos_vals = jnp.cos(angles)[:, None, :]
    sin_vals = jnp.sin(angles)[:, None, :]
    upcast = values_in.astype(jnp.float32)
    front_half = upcast[..., :half_size]
    back_half = upcast[..., half_size:]
    return jnp.concatenate(
        [
            front_half * cos_vals - back_half * sin_vals,
            back_half * cos_vals + front_half * sin_vals,
        ],
        axis=-1,
    )


def shards(
    tokens,
    query_weight,
    key_weight,
    value_weight,
    gate_weight,
    query_gain,
    key_gain,
    out_weight,
    shared_block,
    chosen_device,
):
    tok_rows = tokens.shape[0]
    head_size = query_gain.shape[0]
    head_count = query_weight.shape[1] // head_size
    groups = key_weight.shape[1] // head_size
    per_group = head_count // groups
    group_width = groups * head_size
    block_len = SEL
    local_blocks = tok_rows // block_len
    device = lax.axis_index(KV)
    tp_index = lax.axis_index("tp")
    score_scale = head_size ** (-0.5)
    places = device * tok_rows + jnp.arange(tok_rows, dtype=jnp.int32)
    queries = rounded(jnp.dot(tokens, query_weight, preferred_element_type=jnp.float32)).reshape(
        tok_rows, head_count, head_size
    )
    keys_raw = rounded(jnp.dot(tokens, key_weight, preferred_element_type=jnp.float32)).reshape(
        tok_rows, groups, head_size
    )
    values_raw = rounded(jnp.dot(tokens, value_weight, preferred_element_type=jnp.float32))
    q_plain = rounded(unit_norm(queries, query_gain))
    k_plain = rounded(unit_norm(keys_raw, key_gain))
    q_turned = rotate(q_plain, places).astype(jnp.bfloat16)
    k_turned = rotate(k_plain, places).astype(jnp.bfloat16).reshape(tok_rows, group_width)
    gate_cols = lax.dynamic_slice_in_dim(gate_weight, tp_index * 2 * head_count, 2 * head_count, 1)
    gate_vals = jax.nn.sigmoid(
        jnp.dot(tokens, gate_cols, preferred_element_type=jnp.float32)
    ).reshape(tok_rows, head_count, 2)
    span_count = tok_rows // CMP
    span_keys = jnp.mean(
        k_plain.astype(jnp.float32).reshape(span_count, CMP, group_width), axis=1
    ).astype(jnp.bfloat16)
    span_values = jnp.mean(
        values_raw.astype(jnp.float32).reshape(span_count, CMP, group_width), axis=1
    ).astype(jnp.bfloat16)
    summary = jnp.concatenate([span_keys, span_values], axis=1)
    first_row = shared_block[0] * block_len
    shared = jnp.concatenate(
        [
            lax.dynamic_slice_in_dim(k_turned, first_row, block_len, 0),
            lax.dynamic_slice_in_dim(values_raw, first_row, block_len, 0),
        ],
        axis=1,
    )
    far_count, near_count, y_count = (lax.axis_size(axis) for axis in KV)
    column = spread(spread(jnp.concatenate([shared, summary], axis=0), "z_far"), "z_near")
    column = column.reshape(near_count * far_count, block_len + span_count, 2 * group_width)
    all_summary = spread(column[:, block_len:], "y").reshape(-1, 2 * group_width)
    all_shared = spread(column[:, :block_len], "y").reshape(-1, block_len, 2 * group_width)
    total_spans = all_summary.shape[0]
    slot_of = jnp.arange(total_spans, dtype=jnp.int32) // span_count
    owner = (
        (slot_of % far_count) * near_count + slot_of // far_count % near_count
    ) * y_count + slot_of // (far_count * near_count)
    span_starts = owner * tok_rows + jnp.arange(total_spans, dtype=jnp.int32) % span_count * CMP
    slots = (chosen_device % y_count * near_count + chosen_device // y_count % near_count) * (
        far_count
    ) + chosen_device // (y_count * near_count)
    span_keys_all = all_summary[:, :group_width].reshape(total_spans, groups, head_size)
    span_values_all = all_summary[:, group_width:].reshape(total_spans, groups, head_size)
    q_grouped = q_plain.reshape(tok_rows, groups, per_group, head_size)
    scores = (
        jnp.einsum("rghd,cgd->rghc", q_grouped, span_keys_all, preferred_element_type=jnp.float32)
        * score_scale
    )
    span_ends = span_starts + CMP - 1
    allowed = (span_ends[None, :] <= places[:, None])[:, None, None, :]
    has_span = (places >= CMP - 1)[:, None, None]
    peak_val = jnp.max(jnp.where(allowed, scores, big_negative), axis=-1)
    weights_raw = jnp.where(allowed, jnp.exp(scores - peak_val[..., None]), 0.0)
    divisor = jnp.where(has_span, jnp.sum(weights_raw, axis=-1), 1.0)
    span_out = (
        jnp.einsum(
            "rghc,cgd->rghd",
            weights_raw.astype(jnp.bfloat16),
            span_values_all,
            preferred_element_type=jnp.float32,
        )
        / divisor[..., None]
    )
    span_lse = jnp.where(has_span, peak_val + jnp.log(divisor), 0.0)
    q_blocks = q_turned.reshape(local_blocks, block_len, groups, per_group, head_size)
    own_keys = k_turned.reshape(local_blocks, block_len, groups, head_size)
    own_values = values_raw.reshape(local_blocks, block_len, groups, head_size)
    causal_own = jnp.arange(block_len)[None, :] <= jnp.arange(block_len)[:, None]
    named_count = chosen_device.shape[1]
    remote = all_shared[slots].reshape(
        local_blocks, named_count * block_len, 2 * group_width
    )
    key_rows = jnp.concatenate(
        [own_keys, remote[..., :group_width].reshape(local_blocks, -1, groups, head_size)], axis=1
    )
    value_rows = jnp.concatenate(
        [own_values, remote[..., group_width:].reshape(local_blocks, -1, groups, head_size)], axis=1
    )
    remote_ok = jnp.repeat(chosen_device < device, block_len, axis=1)
    allowed_sel = jnp.concatenate(
        [
            jnp.broadcast_to(causal_own[None], (local_blocks, block_len, block_len)),
            jnp.broadcast_to(
                remote_ok[:, None, :], (local_blocks, block_len, named_count * block_len)
            ),
        ],
        axis=2,
    )[:, :, None, None, :]
    scores_sel = (
        jnp.einsum("jqghd,jkgd->jqghk", q_blocks, key_rows, preferred_element_type=jnp.float32)
        * score_scale
    )
    peak_sel = jnp.max(jnp.where(allowed_sel, scores_sel, big_negative), axis=-1)
    weights_sel = jnp.where(allowed_sel, jnp.exp(scores_sel - peak_sel[..., None]), 0.0)
    sum_sel = jnp.sum(weights_sel, axis=-1)
    chosen_out = (
        jnp.einsum(
            "jqghk,jkgd->jqghd",
            weights_sel.astype(jnp.bfloat16),
            value_rows,
            preferred_element_type=jnp.float32,
        )
        / sum_sel[..., None]
    )
    chosen_lse = peak_sel + jnp.log(sum_sel)
    mixed_heads = (
        gate_vals[..., 0:1] * span_out.reshape(tok_rows, head_count, head_size)
        + gate_vals[..., 1:2] * chosen_out.reshape(tok_rows, head_count, head_size)
    ).astype(jnp.bfloat16)
    mixed_heads = mixed_heads.reshape(tok_rows, head_count * head_size)
    mixed_out = sent_and_summed(
        jnp.dot(mixed_heads, out_weight, preferred_element_type=jnp.float32).astype(jnp.bfloat16),
        "tp",
        0,
    ).astype(jnp.bfloat16)
    log_weight = jnp.stack(
        [span_lse.reshape(tok_rows, head_count), chosen_lse.reshape(tok_rows, head_count)]
    )
    return (mixed_out, log_weight)


def solution(mesh):
    torus = Mesh(mesh.devices.reshape(8, 4, 4, mesh.shape["tp"]), KV_TP)
    return jax.shard_map(
        shards,
        mesh=torus,
        in_specs=(
            P(KV, None),
            P(None, "tp"),
            P(None, "tp"),
            P(None, "tp"),
            P(),
            P(),
            P(),
            P("tp", None),
            P(KV),
            P(KV, None),
        ),
        out_specs=(P(KV_TP, None), P(None, KV, "tp")),
        check_vma=False,
    )
```

```python
import jax
import jax.numpy as jnp
from jax import lax
from jax.experimental import pallas as pl
from jax.experimental.pallas import tpu as pltpu
from jax.sharding import Mesh
from jax.sharding import PartitionSpec as P

SEL = 64
CMP = 32
KV = ("z_far", "z_near", "y")
KV_TP = ("z_far", "z_near", "y", "tp")


norm_eps = 1e-06
rope_base = 500000.0
big_negative = -1e30


def spread(block, axis):
    count = lax.axis_size(axis)
    copies = lax.optimization_barrier(jnp.broadcast_to(block[None], (count, *block.shape)))
    return lax.all_to_all(copies, axis, split_axis=0, concat_axis=0, tiled=True)


def split_up(array, dim, length):
    lengths = array.shape
    pieces = array.reshape(*lengths[:dim], length, lengths[dim] // length, *lengths[dim + 1 :])
    return jnp.moveaxis(pieces, dim, 0)


def sent_and_summed(array, axis, dim):
    pieces = split_up(array, dim, lax.axis_size(axis))
    arrived = lax.all_to_all(pieces, axis, split_axis=0, concat_axis=0, tiled=True)
    return arrived.astype(jnp.float32).sum(axis=0)


def rounded(values_in):
    return lax.optimization_barrier(values_in.astype(jnp.bfloat16))


def unit_norm(values_in, gain_vec):
    upcast = values_in.astype(jnp.float32)
    return (
        upcast * lax.rsqrt(jnp.mean(upcast * upcast, axis=-1, keepdims=True) + norm_eps) * gain_vec
    )


def rotate(values_in, places):
    half_size = values_in.shape[-1] // 2
    inverse = jnp.power(
        rope_base, -jnp.arange(half_size, dtype=jnp.float32) * 2.0 / values_in.shape[-1]
    )
    angles = places.astype(jnp.float32)[:, None] * inverse[None, :]
    cos_vals = jnp.cos(angles)[:, None, :]
    sin_vals = jnp.sin(angles)[:, None, :]
    upcast = values_in.astype(jnp.float32)
    front_half = upcast[..., :half_size]
    back_half = upcast[..., half_size:]
    return jnp.concatenate(
        [
            front_half * cos_vals - back_half * sin_vals,
            back_half * cos_vals + front_half * sin_vals,
        ],
        axis=-1,
    )


def swapped(values_in):
    half_size = values_in.shape[-1] // 2
    return jnp.concatenate([values_in[:, half_size:], values_in[:, :half_size]], axis=1)


def side_by_side(rows):
    half_size = rows.shape[0] // 2
    return jnp.concatenate([rows[:half_size], rows[half_size:]], axis=1)


def dot_last(left, right):
    return lax.dot_general(
        left, right, (((1,), (1,)), ((), ())), preferred_element_type=jnp.float32
    )


def key_kernel(pick, tokens, key_weight, value_weight, gain, cosines, sines, sent, own_keys, own_values):
    copies, _, _ = sent.shape
    blocks, packed, _ = own_keys.shape
    tok_rows = tokens.shape[0]
    block_len = 2 * packed
    keys = dot_last(tokens[...], key_weight[...])
    keys = keys.astype(jnp.bfloat16).astype(jnp.float32)
    values = dot_last(tokens[...], value_weight[...]).astype(jnp.bfloat16)
    square = jnp.mean(keys * keys, axis=-1, keepdims=True)
    plain = (keys * lax.rsqrt(square + norm_eps) * gain[...]).astype(jnp.bfloat16)
    plain = plain.astype(jnp.float32)
    turned = (plain * cosines[...] + swapped(plain) * sines[...]).astype(jnp.bfloat16)
    for block in range(blocks):
        rows = slice(block * block_len, (block + 1) * block_len)
        own_keys[block] = side_by_side(turned[rows])
        own_values[block] = side_by_side(values[rows])
    both = jnp.concatenate([plain, values.astype(jnp.float32)], axis=1)
    spans = jnp.mean(both.reshape(tok_rows // CMP, CMP, both.shape[1]), axis=1).astype(jnp.bfloat16)
    shared_keys = own_keys[pick[0]]
    shared_values = own_values[pick[0]]
    for copy in range(copies):
        sent[copy, :packed] = shared_keys
        sent[copy, packed:block_len] = shared_values
        sent[copy, block_len:] = spans


def one_sided(queries, rows, upper):
    pieces = []
    lanes = lax.broadcasted_iota(jnp.int32, (rows.size, 128), 1)
    keep = (lanes >= 64) if upper else (lanes < 64)
    for pair in range(queries.shape[1] // 128):
        both = queries[rows, pair * 128 : (pair + 1) * 128].astype(jnp.float32)
        turned = swapped(both)
        for piece in (turned, both) if upper else (both, turned):
            pieces.append(jnp.where(keep, piece, 0.0).astype(jnp.bfloat16))
    return jnp.concatenate(pieces, axis=0)


def score_kernel(
    starts,
    origin,
    blocked,
    span_ends,
    arrived,
    own_keys,
    q_plain,
    q_turned,
    gates,
    weights,
    mixed_spans,
    factors,
    logs,
    chosen_keys,
    spans,
):
    blocks, packed, _ = own_keys.shape
    y_count, arrived_rows, _ = arrived.shape
    block_len = 2 * packed
    heads = q_plain.shape[1] // 64
    named = starts.shape[0] // blocks
    span_rows = spans.shape[0] // y_count
    score_scale = 64 ** (-0.5)
    for place in range(y_count):
        spans[place * span_rows : (place + 1) * span_rows] = arrived[
            place, arrived_rows - span_rows :
        ]
    row_place = lax.broadcasted_iota(jnp.int32, (heads * block_len, 1), 0) % block_len

    @pl.loop(0, blocks)
    def _(block):
        rows = pl.ds(pl.multiple_of(block * block_len, block_len), block_len)
        gate_rows = gates[rows, :]
        gate_of = [
            jnp.concatenate(
                [gate_rows[:, 2 * head + b : 2 * head + b + 1] for head in range(heads)], axis=0
            )
            for b in range(2)
        ]
        scores = dot_last(one_sided(q_plain, rows, False), spans[...])
        places = origin[0] + block * block_len + row_place
        has_span = places >= CMP - 1
        scores = jnp.where(span_ends[...] <= places, scores * score_scale, big_negative)
        peak = jnp.max(scores, axis=-1, keepdims=True)
        raw = jnp.exp(scores - peak)
        total = jnp.where(has_span, jnp.sum(raw, axis=-1, keepdims=True), 1.0)
        summed = jnp.dot(raw.astype(jnp.bfloat16), spans[...], preferred_element_type=jnp.float32)
        summed = jnp.where(has_span, gate_of[0] * (summed[:, 64:] / total), 0.0)
        span_log = jnp.where(has_span, peak + jnp.log(total), 0.0)
        for pair in range(heads // 2):
            first = slice(2 * pair * block_len, (2 * pair + 1) * block_len)
            second = slice((2 * pair + 1) * block_len, (2 * pair + 2) * block_len)
            mixed_spans[rows, pair * 128 : (pair + 1) * 128] = jnp.concatenate(
                [summed[first], summed[second]], axis=1
            )
        chosen_keys[:packed] = own_keys[block]
        for number in range(named):
            start = pl.multiple_of(starts[block * named + number], packed)
            place = start // arrived_rows
            chosen_keys[(number + 1) * packed : (number + 2) * packed] = arrived[
                place, pl.ds(pl.multiple_of(start - place * arrived_rows, packed), packed)
            ]
        half_scores = []
        lanes = lax.broadcasted_iota(jnp.int32, (heads * block_len, chosen_keys.shape[0]), 1)
        for upper in (False, True):
            scores = dot_last(one_sided(q_turned, rows, upper), chosen_keys[...])
            scores = scores * score_scale + blocked[block]
            later = (lanes < packed) & (lanes + packed * upper > row_place)
            half_scores.append(jnp.where(later, big_negative, scores))
        peak = jnp.maximum(
            jnp.max(half_scores[0], axis=-1, keepdims=True),
            jnp.max(half_scores[1], axis=-1, keepdims=True),
        )
        total = 0.0
        for upper in range(2):
            raw = jnp.exp(half_scores[upper] - peak)
            total = total + jnp.sum(raw, axis=-1, keepdims=True)
            weights[block, upper] = raw.astype(jnp.bfloat16)
        factors[block] = jnp.broadcast_to(gate_of[1] / total, factors.shape[1:])
        chosen_log = peak + jnp.log(total)
        for head in range(heads):
            piece = slice(head * block_len, (head + 1) * block_len)
            logs[0, rows, head : head + 1] = span_log[piece]
            logs[1, rows, head : head + 1] = chosen_log[piece]


def mix_kernel(starts, arrived, own_values, weights, mixed_spans, factors, mixed, chosen_values):
    blocks, packed, _ = own_values.shape
    block_len = 2 * packed
    named = starts.shape[0] // blocks
    heads = factors.shape[1] // block_len

    @pl.loop(0, blocks)
    def _(block):
        rows = pl.ds(pl.multiple_of(block * block_len, block_len), block_len)
        chosen_values[:packed] = own_values[block]
        for number in range(named):
            start = pl.multiple_of(starts[block * named + number], packed)
            chosen_values[(number + 1) * packed : (number + 2) * packed] = arrived[
                pl.ds(start, packed)
            ]
        lower, upper = (
            jnp.dot(weights[block, half], chosen_values[...], preferred_element_type=jnp.float32)
            for half in range(2)
        )
        summed = (lower + swapped(upper)) * factors[block]
        for pair in range(heads // 2):
            first = summed[2 * pair * block_len : (2 * pair + 1) * block_len, :64]
            second = summed[(2 * pair + 1) * block_len : (2 * pair + 2) * block_len, :64]
            lane_range = slice(pair * 128, (pair + 1) * 128)
            mixed[rows, lane_range] = (
                mixed_spans[rows, lane_range] + jnp.concatenate([first, second], axis=1)
            ).astype(jnp.bfloat16)


def in_vmem(kernel, scalars, arrays, outputs, scratch, flops, room):
    return pl.pallas_call(
        kernel,
        out_shape=outputs,
        in_specs=[pl.BlockSpec(memory_space=pltpu.SMEM)] * len(scalars)
        + [pl.BlockSpec(memory_space=pltpu.VMEM)] * len(arrays),
        out_specs=jax.tree.map(lambda _: pl.BlockSpec(memory_space=pltpu.VMEM), outputs),
        scratch_shapes=scratch,
        cost_estimate=pl.CostEstimate(flops=flops, bytes_accessed=4 << 20, transcendentals=0),
        compiler_params=pltpu.CompilerParams(vmem_limit_bytes=room << 20),
    )(*scalars, *arrays)


def turns(places, head_size):
    half_size = head_size // 2
    inverse = jnp.power(rope_base, -jnp.arange(half_size, dtype=jnp.float32) * 2.0 / head_size)
    angles = places.astype(jnp.float32)[:, None] * inverse[None, :]
    return jnp.cos(angles), jnp.sin(angles)


def shards(
    tokens,
    query_weight,
    key_weight,
    value_weight,
    gate_weight,
    query_gain,
    key_gain,
    out_weight,
    shared_block,
    chosen_device,
):
    tok_rows = tokens.shape[0]
    head_size = query_gain.shape[0]
    head_count = query_weight.shape[1] // head_size
    block_len = SEL
    packed = block_len // 2
    local_blocks = tok_rows // block_len
    device = lax.axis_index(KV)
    tp_index = lax.axis_index("tp")
    places = device * tok_rows + jnp.arange(tok_rows, dtype=jnp.int32)
    far_count, near_count, y_count = (lax.axis_size(axis) for axis in KV)
    column_count = far_count * near_count
    span_count = tok_rows // CMP
    cos_vals, sin_vals = turns(places, head_size)

    packed_blocks = jax.ShapeDtypeStruct((local_blocks, packed, 2 * head_size), jnp.bfloat16)
    sent, own_keys, own_values = in_vmem(
        key_kernel,
        (shared_block,),
        (
            tokens,
            key_weight.T,
            value_weight.T,
            key_gain[None],
            jnp.concatenate([cos_vals, cos_vals], axis=1),
            jnp.concatenate([-sin_vals, sin_vals], axis=1),
        ),
        (
            jax.ShapeDtypeStruct(
                (far_count, block_len + span_count, 2 * head_size), jnp.bfloat16
            ),
            packed_blocks,
            packed_blocks,
        ),
        (),
        10**9,
        8,
    )
    far = lax.all_to_all(sent, "z_far", split_axis=0, concat_axis=0, tiled=True)
    column = spread(far, "z_near").reshape(column_count, block_len + span_count, 2 * head_size)
    first_part = jnp.concatenate(
        [
            column[:, :packed].reshape(-1, 2 * head_size),
            column[:, block_len:].reshape(-1, 2 * head_size),
        ],
        axis=0,
    )
    arrived_keys = spread(first_part, "y")
    arrived_values = spread(column[:, packed:block_len].reshape(-1, 2 * head_size), "y")
    arrived_values = arrived_values.reshape(-1, 2 * head_size)

    queries = rounded(jnp.dot(tokens, query_weight, preferred_element_type=jnp.float32)).reshape(
        tok_rows, head_count, head_size
    )
    q_plain = rounded(unit_norm(queries, query_gain))
    q_turned = rotate(q_plain, places).astype(jnp.bfloat16)
    gate_cols = lax.dynamic_slice_in_dim(gate_weight, tp_index * 2 * head_count, 2 * head_count, 1)
    gate_vals = jax.nn.sigmoid(jnp.dot(tokens, gate_cols, preferred_element_type=jnp.float32))

    span_index = jnp.arange(y_count * column_count * span_count, dtype=jnp.int32)
    slot_of = span_index // span_count
    owner = (
        (slot_of % far_count) * near_count + slot_of // far_count % near_count
    ) * y_count + slot_of // column_count
    span_ends = owner * tok_rows + span_index % span_count * CMP + CMP - 1
    in_column = chosen_device // y_count % near_count * far_count + chosen_device // (
        y_count * near_count
    )
    place = chosen_device % y_count
    key_starts = (place * first_part.shape[0] + in_column * packed).reshape(-1)
    value_starts = ((place * column_count + in_column) * packed).reshape(-1)
    counted = jnp.concatenate(
        [jnp.ones((local_blocks, 1), jnp.bool_), chosen_device < device], axis=1
    )
    blocked = jnp.repeat(jnp.where(counted, 0.0, big_negative), packed, axis=1)[:, None, :]
    chosen_rows = blocked.shape[2]

    weights, mixed_spans, factors, log_weight = in_vmem(
        score_kernel,
        (key_starts, (device * tok_rows)[None]),
        (
            blocked,
            span_ends[None],
            arrived_keys,
            own_keys,
            q_plain.reshape(tok_rows, head_count * head_size),
            q_turned.reshape(tok_rows, head_count * head_size),
            gate_vals,
        ),
        (
            jax.ShapeDtypeStruct(
                (local_blocks, 2, head_count * block_len, chosen_rows), jnp.bfloat16
            ),
            jax.ShapeDtypeStruct((tok_rows, head_count * head_size), jnp.float32),
            jax.ShapeDtypeStruct(
                (local_blocks, head_count * block_len, 2 * head_size), jnp.float32
            ),
            jax.ShapeDtypeStruct((2, tok_rows, head_count), jnp.float32),
        ),
        (
            pltpu.VMEM((chosen_rows, 2 * head_size), jnp.bfloat16),
            pltpu.VMEM((span_ends.shape[0], 2 * head_size), jnp.bfloat16),
        ),
        4 * 10**9,
        16,
    )
    mixed_heads = in_vmem(
        mix_kernel,
        (value_starts,),
        (arrived_values, own_values, weights, mixed_spans, factors),
        jax.ShapeDtypeStruct((tok_rows, head_count * head_size), jnp.bfloat16),
        (pltpu.VMEM((chosen_rows, 2 * head_size), jnp.bfloat16),),
        10**9,
        10,
    )
    mixed_out = sent_and_summed(
        jnp.dot(mixed_heads, out_weight, preferred_element_type=jnp.float32).astype(jnp.bfloat16),
        "tp",
        0,
    ).astype(jnp.bfloat16)
    return (mixed_out, log_weight)


def solution(mesh):
    torus = Mesh(mesh.devices.reshape(8, 4, 4, mesh.shape["tp"]), KV_TP)
    return jax.shard_map(
        shards,
        mesh=torus,
        in_specs=(
            P(KV, None),
            P(None, "tp"),
            P(None, "tp"),
            P(None, "tp"),
            P(),
            P(),
            P(),
            P("tp", None),
            P(KV),
            P(KV, None),
        ),
        out_specs=(P(KV_TP, None), P(None, KV, "tp")),
        check_vma=False,
    )
```

```python
import jax
import jax.numpy as jnp
from jax import lax
from jax.experimental import pallas as pl
from jax.experimental.pallas import tpu as pltpu
from jax.sharding import Mesh
from jax.sharding import PartitionSpec as P

SEL = 64
CMP = 32
KV = ("z", "y")
TP = ("x", "core")
KEY_ROOM = 60
QUERY_ROOM = 60
ATTENTION_ROOM = 12


norm_eps = 1e-06
rope_base = 500000.0
big_negative = -1e30


def spread(block, axis):
    count = lax.axis_size(axis)
    copies = lax.optimization_barrier(jnp.broadcast_to(block[None], (count, *block.shape)))
    return lax.all_to_all(copies, axis, split_axis=0, concat_axis=0, tiled=True)


def swapped(values_in):
    half_size = values_in.shape[-1] // 2
    return jnp.concatenate([values_in[:, half_size:], values_in[:, :half_size]], axis=1)


def side_by_side(rows):
    half_size = rows.shape[0] // 2
    return jnp.concatenate([rows[:half_size], rows[half_size:]], axis=1)


def dot_last(left, right):
    return lax.dot_general(
        left, right, (((1,), (1,)), ((), ())), preferred_element_type=jnp.float32
    )


def key_kernel(pick, tokens, key_weight, value_weight, gain, cosines, sines, sent, own):
    _, blocks, packed, _ = own.shape
    tok_rows = tokens.shape[0]
    block_len = 2 * packed
    keys = dot_last(tokens[...], key_weight[...])
    keys = keys.astype(jnp.bfloat16).astype(jnp.float32)
    values = dot_last(tokens[...], value_weight[...]).astype(jnp.bfloat16)
    square = jnp.mean(keys * keys, axis=-1, keepdims=True)
    plain = (keys * lax.rsqrt(square + norm_eps) * gain[...]).astype(jnp.bfloat16)
    plain = plain.astype(jnp.float32)
    turned = plain * cosines[:, :64] + swapped(plain) * sines[:, :64]
    turned = turned.astype(jnp.bfloat16)
    for block in range(blocks):
        rows = slice(block * block_len, (block + 1) * block_len)
        own[0, block] = side_by_side(turned[rows])
        own[1, block] = side_by_side(values[rows])
    both = jnp.concatenate([plain, values.astype(jnp.float32)], axis=1)
    spans = jnp.mean(both.reshape(tok_rows // CMP, CMP, both.shape[1]), axis=1)
    sent[:packed] = own[0, pick[0]]
    sent[packed:block_len] = own[1, pick[0]]
    sent[block_len:] = spans.astype(jnp.bfloat16)


def query_kernel(group, tokens, query_weight, gate_weight, gain, cosines, sines, ready, gates):
    tok_rows = tokens.shape[0]
    width = query_weight.shape[1]
    gate_count = gates.shape[1]
    start = pl.multiple_of(group[0] * gate_count, gate_count)
    gates[...] = jax.nn.sigmoid(
        dot_last(tokens[...], gate_weight[pl.ds(start, gate_count), :].astype(jnp.bfloat16))
    )
    lanes = lax.broadcasted_iota(jnp.int32, (tok_rows, 128), 1)
    for pair in range(width // 128):
        queries = jnp.dot(
            tokens[...],
            query_weight[:, pair * 128 : (pair + 1) * 128],
            preferred_element_type=jnp.float32,
        )
        queries = queries.astype(jnp.bfloat16).astype(jnp.float32)
        squares = queries * queries
        first = jnp.sum(jnp.where(lanes < 64, squares, 0.0), axis=-1, keepdims=True)
        second = jnp.sum(jnp.where(lanes < 64, 0.0, squares), axis=-1, keepdims=True)
        square = jnp.where(lanes < 64, first, second) * (1.0 / 64)
        plain = (queries * lax.rsqrt(square + norm_eps) * gain[...]).astype(jnp.bfloat16)
        ready[0, pair] = plain
        plain = plain.astype(jnp.float32)
        partner = jnp.where(
            lanes % 64 < 32, pltpu.roll(plain, 96, axis=1), pltpu.roll(plain, 32, axis=1)
        )
        turned = plain * cosines[...] + partner * sines[...]
        ready[1, pair] = turned.astype(jnp.bfloat16)


def one_sided(queries, upper):
    pieces = []
    lanes = lax.broadcasted_iota(jnp.int32, queries[0].shape, 1)
    keep = (lanes >= 64) if upper else (lanes < 64)
    for both in queries:
        both = both.astype(jnp.float32)
        turned = swapped(both)
        for piece in (turned, both) if upper else (both, turned):
            pieces.append(jnp.where(keep, piece, 0.0).astype(jnp.bfloat16))
    return jnp.concatenate(pieces, axis=0)


def attention_kernel(
    place_of,
    chosen,
    arrived,
    ready_far,
    gates_far,
    own_far,
    kept,
    given,
    logs,
    ready,
    gates,
    own,
    chosen_rows,
    spans,
    semaphores,
):
    device, core = place_of[0], place_of[1]
    blocks, named = chosen.shape
    _, _, packed, _ = own.shape
    y_count, z_count, sent_rows, _ = arrived.shape
    block_len = 2 * packed
    pairs = ready.shape[1]
    heads = 2 * pairs
    tok_rows = blocks * block_len
    span_rows = sent_rows - block_len
    score_scale = 64 ** (-0.5)
    loads = [
        pltpu.make_async_copy(far, near, semaphores.at[number])
        for number, (far, near) in enumerate(
            ((ready_far, ready), (gates_far, gates), (own_far, own))
        )
    ]
    for load in loads:
        load.start()
    column_rows = z_count * span_rows
    for y in range(y_count):
        column = arrived[y, :, block_len:, :].astype(jnp.float32)
        spans[y * column_rows : (y + 1) * column_rows] = column.reshape(column_rows, 128).astype(
            jnp.bfloat16
        )
    for load in loads:
        load.wait()
    row_place = lax.broadcasted_iota(jnp.int32, (heads * block_len, 1), 0) % block_len
    span_index = lax.broadcasted_iota(jnp.int32, (1, y_count * column_rows), 1)
    owner = span_index % column_rows // span_rows * y_count + span_index // column_rows
    span_ends = owner * tok_rows + span_index % span_rows * CMP + CMP - 1
    rank = lax.broadcasted_iota(jnp.int32, (1, chosen_rows.shape[1]), 1) // packed

    @pl.loop(0, blocks)
    def _(block):
        rows = pl.ds(pl.multiple_of(block * block_len, block_len), block_len)
        gate_rows = gates[rows, :]
        gate_of = [
            jnp.concatenate(
                [gate_rows[:, 2 * head + b : 2 * head + b + 1] for head in range(heads)], axis=0
            )
            for b in range(2)
        ]
        scores = dot_last(
            one_sided([ready[0, pair, rows, :] for pair in range(pairs)], False), spans[...]
        )
        places = device * tok_rows + block * block_len + row_place
        has_span = places >= CMP - 1
        scores = jnp.where(span_ends <= places, scores * score_scale, big_negative)
        peak = jnp.max(scores, axis=-1, keepdims=True)
        raw = jnp.exp(scores - peak)
        total = jnp.where(has_span, jnp.sum(raw, axis=-1, keepdims=True), 1.0)
        summed = jnp.dot(raw.astype(jnp.bfloat16), spans[...], preferred_element_type=jnp.float32)
        mixed_spans = jnp.where(has_span, gate_of[0] * (summed[:, 64:] / total), 0.0)
        span_log = jnp.where(has_span, peak + jnp.log(total), 0.0)

        blocked = jnp.zeros(rank.shape, jnp.float32)
        for part in range(2):
            chosen_rows[part, :packed] = own[part, block]
        for number in range(named):
            source = chosen[block, number]
            z, y = source // y_count, source % y_count
            for part in range(2):
                chosen_rows[part, (number + 1) * packed : (number + 2) * packed] = arrived[
                    y, z, part * packed : (part + 1) * packed, :
                ]
            bias = jnp.where(source < device, 0.0, big_negative)
            blocked = jnp.where(rank == number + 1, bias, blocked)
        half_scores = []
        lanes = lax.broadcasted_iota(jnp.int32, (heads * block_len, chosen_rows.shape[1]), 1)
        queries = [ready[1, pair, rows, :] for pair in range(pairs)]
        for upper in (False, True):
            scores = dot_last(one_sided(queries, upper), chosen_rows[0])
            scores = scores * score_scale + blocked
            later = (lanes < packed) & (lanes + packed * upper > row_place)
            half_scores.append(jnp.where(later, big_negative, scores))
        peak = jnp.maximum(
            jnp.max(half_scores[0], axis=-1, keepdims=True),
            jnp.max(half_scores[1], axis=-1, keepdims=True),
        )
        total = 0.0
        products = []
        for upper in range(2):
            raw = jnp.exp(half_scores[upper] - peak)
            total = total + jnp.sum(raw, axis=-1, keepdims=True)
            products.append(
                jnp.dot(
                    raw.astype(jnp.bfloat16), chosen_rows[1], preferred_element_type=jnp.float32
                )
            )
        summed = products[0][:, :64] + products[1][:, 64:]
        mixed = mixed_spans + gate_of[1] * (summed / total)
        chosen_log = peak + jnp.log(total)
        for pair in range(pairs):
            first = mixed[2 * pair * block_len : (2 * pair + 1) * block_len]
            second = mixed[(2 * pair + 1) * block_len : (2 * pair + 2) * block_len]
            both = jnp.concatenate([first, second], axis=1)
            lower, upper = both[:packed], both[packed:]
            lane_range = slice(pair * 128, (pair + 1) * 128)
            kept[block, :, lane_range] = jnp.where(core == 0, lower, upper).astype(jnp.bfloat16)
            given[block, :, lane_range] = jnp.where(core == 0, upper, lower).astype(jnp.bfloat16)
        for head in range(heads):
            piece = slice(head * block_len, (head + 1) * block_len)
            logs[0, rows, head : head + 1] = span_log[piece]
            logs[1, rows, head : head + 1] = chosen_log[piece]


def kernel_call(kernel, specs, operands, outputs, scratch, flops, room):
    return pl.pallas_call(
        kernel,
        out_shape=outputs,
        in_specs=[pl.BlockSpec(memory_space=space) for space in specs],
        out_specs=jax.tree.map(lambda _: pl.BlockSpec(memory_space=pltpu.VMEM), outputs),
        scratch_shapes=scratch,
        cost_estimate=pl.CostEstimate(flops=flops, bytes_accessed=4 << 20, transcendentals=0),
        compiler_params=pltpu.CompilerParams(vmem_limit_bytes=room << 20),
    )(*operands)


def turns(places, head_size):
    half_size = head_size // 2
    inverse = jnp.power(rope_base, -jnp.arange(half_size, dtype=jnp.float32) * 2.0 / head_size)
    angles = places.astype(jnp.float32)[:, None] * inverse[None, :]
    cos_vals, sin_vals = jnp.cos(angles), jnp.sin(angles)
    return (
        jnp.concatenate([cos_vals] * 4, axis=1),
        jnp.concatenate([-sin_vals, sin_vals] * 2, axis=1),
    )


def shards(
    tokens,
    query_weight,
    key_weight,
    value_weight,
    gate_weight,
    query_gain,
    key_gain,
    out_weight,
    shared_block,
    chosen_device,
):
    tok_rows = tokens.shape[0]
    head_size = query_gain.shape[0]
    width = query_weight.shape[1]
    head_count = width // head_size
    packed = SEL // 2
    local_blocks = tok_rows // SEL
    device = lax.axis_index(KV)
    z_count, y_count = (lax.axis_size(axis) for axis in KV)
    sent_rows = SEL + tok_rows // CMP
    places = device * tok_rows + jnp.arange(tok_rows, dtype=jnp.int32)
    cosines, sines = turns(places, head_size)
    bf16, f32 = jnp.bfloat16, jnp.float32
    shape = jax.ShapeDtypeStruct
    vmem, smem, anywhere = pltpu.VMEM, pltpu.SMEM, pl.ANY

    sent, own = kernel_call(
        key_kernel,
        [smem] + [vmem] * 6,
        (shared_block, tokens, key_weight.T, value_weight.T, key_gain[None], cosines, sines),
        (shape((sent_rows, 128), bf16), shape((2, local_blocks, packed, 128), bf16)),
        (),
        10**9,
        KEY_ROOM,
    )
    column = lax.all_gather(sent, "z", axis=0, tiled=True)
    arrived = spread(column, "y").reshape(y_count, z_count, sent_rows, 128)

    tokens_later, own, cosines, sines, swap_weight, _ = lax.optimization_barrier(
        (tokens, own, cosines, sines, out_weight, column)
    )
    other_weight = lax.ppermute(swap_weight, "core", [(0, 1), (1, 0)])
    ready, gates = kernel_call(
        query_kernel,
        [smem] + [vmem] * 6,
        (
            lax.axis_index(TP).reshape(1),
            tokens_later,
            query_weight,
            gate_weight.T,
            jnp.concatenate([query_gain, query_gain])[None],
            cosines,
            sines,
        ),
        (
            shape((2, width // 128, tok_rows, 128), bf16),
            shape((tok_rows, 2 * head_count), f32),
        ),
        (),
        10**9,
        QUERY_ROOM,
    )
    kept, given, log_weight = kernel_call(
        attention_kernel,
        [smem, smem, vmem, anywhere, anywhere, anywhere],
        (
            jnp.stack([device, lax.axis_index("core")]),
            chosen_device,
            arrived,
            ready,
            gates,
            own,
        ),
        (
            shape((local_blocks, packed, width), bf16),
            shape((local_blocks, packed, width), bf16),
            shape((2, tok_rows, head_count), f32),
        ),
        (
            pltpu.VMEM(ready.shape, bf16),
            pltpu.VMEM(gates.shape, f32),
            pltpu.VMEM(own.shape, bf16),
            pltpu.VMEM((2, (chosen_device.shape[1] + 1) * packed, 128), bf16),
            pltpu.VMEM((y_count * z_count * (sent_rows - SEL), 128), bf16),
            pltpu.SemaphoreType.DMA((3,)),
        ),
        4 * 10**9,
        ATTENTION_ROOM,
    )
    taken = lax.ppermute(given, "core", [(0, 1), (1, 0)])
    own_partial = jnp.dot(
        kept.reshape(-1, width), out_weight, preferred_element_type=jnp.float32
    ).astype(bf16)
    other_partial = jnp.dot(
        taken.reshape(-1, width), other_weight, preferred_element_type=jnp.float32
    ).astype(bf16)
    pair_sum = (own_partial.astype(f32) + other_partial.astype(f32)).astype(bf16)
    pair_sum = pair_sum.reshape(local_blocks, packed, -1)
    pieces = lax.all_to_all(pair_sum, "x", split_axis=0, concat_axis=0, tiled=True)
    mixed_out = pieces.astype(f32).sum(axis=0).astype(bf16)
    return (mixed_out, log_weight)


def solution(mesh):
    torus = Mesh(mesh.devices.reshape(32, 4, 4, 2), ("z", "y", "x", "core"))
    return jax.shard_map(
        shards,
        mesh=torus,
        in_specs=(
            P(KV, None),
            P(None, TP),
            P(None, TP),
            P(None, TP),
            P(),
            P(),
            P(),
            P(TP, None),
            P(KV),
            P(KV, None),
        ),
        out_specs=(P((*KV, *TP), None), P(None, KV, TP)),
        check_vma=False,
    )
```

```python
import functools

import jax
import jax.numpy as jnp
from jax import lax
from jax.experimental import pallas as pl
from jax.experimental.pallas import tpu as pltpu
from jax.sharding import Mesh
from jax.sharding import PartitionSpec as P

SEL = 64
CMP = 32
KV = ("z_far", "z_near", "y")
TP = ("x", "core")
KEY_ROOM = 60
QUERY_ROOM = 60
ATTENTION_ROOM = 12


norm_eps = 1e-06
rope_base = 500000.0
big_negative = -1e30


def spread(block, axis):
    count = lax.axis_size(axis)
    copies = lax.optimization_barrier(jnp.broadcast_to(block[None], (count, *block.shape)))
    return lax.all_to_all(copies, axis, split_axis=0, concat_axis=0, tiled=True)


def swapped(values_in):
    half_size = values_in.shape[-1] // 2
    return jnp.concatenate([values_in[:, half_size:], values_in[:, :half_size]], axis=1)


def repeated(halves, signs):
    return jnp.concatenate([sign * halves for sign in signs], axis=1)


def side_by_side(rows):
    half_size = rows.shape[0] // 2
    return jnp.concatenate([rows[:half_size], rows[half_size:]], axis=1)


def dot_last(left, right):
    return lax.dot_general(
        left, right, (((1,), (1,)), ((), ())), preferred_element_type=jnp.float32
    )


def key_kernel(pick, tokens, key_weight, value_weight, gain, cosines, sines, sent, own):
    _, blocks, packed, _ = own.shape
    tok_rows = tokens.shape[0]
    block_len = 2 * packed
    keys = dot_last(tokens[...], key_weight[...])
    keys = keys.astype(jnp.bfloat16).astype(jnp.float32)
    values = dot_last(tokens[...], value_weight[...]).astype(jnp.bfloat16)
    square = jnp.mean(keys * keys, axis=-1, keepdims=True)
    plain = (keys * lax.rsqrt(square + norm_eps) * gain[...]).astype(jnp.bfloat16)
    plain = plain.astype(jnp.float32)
    turned = plain * repeated(cosines[...], (1, 1)) + swapped(plain) * repeated(
        sines[...], (-1, 1)
    )
    turned = turned.astype(jnp.bfloat16)
    for block in range(blocks):
        rows = slice(block * block_len, (block + 1) * block_len)
        own[0, block] = side_by_side(turned[rows])
        own[1, block] = side_by_side(values[rows])
    both = jnp.concatenate([plain, values.astype(jnp.float32)], axis=1)
    spans = jnp.mean(both.reshape(tok_rows // CMP, CMP, both.shape[1]), axis=1)
    sent[:packed] = own[0, pick[0]]
    sent[packed:block_len] = own[1, pick[0]]
    sent[block_len:] = spans.astype(jnp.bfloat16)


def query_kernel(group, tokens, query_weight, gate_weight, gain, cosines, sines, ready):
    tok_rows = tokens.shape[0]
    width = query_weight.shape[1]
    gate_count = 2 * (width // 64)
    start = pl.multiple_of(group[0] * gate_count, gate_count)
    ready[2 * (width // 128), :, :gate_count] = jax.nn.sigmoid(
        dot_last(tokens[...], gate_weight[pl.ds(start, gate_count), :].astype(jnp.bfloat16))
    )
    lanes = lax.broadcasted_iota(jnp.int32, (tok_rows, 128), 1)
    cos_lanes = repeated(cosines[...], (1, 1, 1, 1))
    sin_lanes = repeated(sines[...], (-1, 1, -1, 1))
    for pair in range(width // 128):
        queries = jnp.dot(
            tokens[...],
            query_weight[:, pair * 128 : (pair + 1) * 128],
            preferred_element_type=jnp.float32,
        )
        queries = queries.astype(jnp.bfloat16).astype(jnp.float32)
        squares = queries * queries
        first = jnp.sum(jnp.where(lanes < 64, squares, 0.0), axis=-1, keepdims=True)
        second = jnp.sum(jnp.where(lanes < 64, 0.0, squares), axis=-1, keepdims=True)
        square = jnp.where(lanes < 64, first, second) * (1.0 / 64)
        plain = (queries * lax.rsqrt(square + norm_eps) * gain[...]).astype(jnp.bfloat16)
        plain = plain.astype(jnp.float32)
        ready[pair] = plain
        partner = jnp.where(
            lanes % 64 < 32, pltpu.roll(plain, 96, axis=1), pltpu.roll(plain, 32, axis=1)
        )
        turned = plain * cos_lanes + partner * sin_lanes
        ready[width // 128 + pair] = turned.astype(jnp.bfloat16).astype(jnp.float32)


def one_sided(queries, upper):
    pieces = []
    lanes = lax.broadcasted_iota(jnp.int32, queries[0].shape, 1)
    keep = (lanes >= 64) if upper else (lanes < 64)
    for both in queries:
        turned = swapped(both)
        for piece in (turned, both) if upper else (both, turned):
            pieces.append(jnp.where(keep, piece, 0.0).astype(jnp.bfloat16))
    return jnp.concatenate(pieces, axis=0)


def attention_kernel(
    far_count,
    place_of,
    chosen,
    arrived,
    ready,
    own,
    kept,
    given,
    logs,
    chosen_rows,
    spans,
):
    device, core = place_of[0], place_of[1]
    blocks, named = chosen.shape
    _, _, packed, _ = own.shape
    y_count, z_count, sent_rows, _ = arrived.shape
    block_len = 2 * packed
    pairs = kept.shape[2] // 128
    heads = 2 * pairs
    tok_rows = blocks * block_len
    span_rows = sent_rows - block_len
    score_scale = 64 ** (-0.5)
    column_rows = z_count * span_rows
    for y in range(y_count):
        column = arrived[y, :, block_len:, :].astype(jnp.float32)
        spans[y * column_rows : (y + 1) * column_rows] = column.reshape(column_rows, 128).astype(
            jnp.bfloat16
        )
    row_place = lax.broadcasted_iota(jnp.int32, (heads * block_len, 1), 0) % block_len
    span_index = lax.broadcasted_iota(jnp.int32, (1, y_count * column_rows), 1)
    slot = span_index % column_rows // span_rows
    near_count = z_count // far_count
    owner = (slot % far_count * near_count + slot // far_count) * y_count
    owner = owner + span_index // column_rows
    span_ends = owner * tok_rows + span_index % span_rows * CMP + CMP - 1
    rank = lax.broadcasted_iota(jnp.int32, (1, chosen_rows.shape[1]), 1) // packed

    @pl.loop(0, blocks)
    def _(block):
        rows = pl.ds(pl.multiple_of(block * block_len, block_len), block_len)
        gate_rows = ready[2 * pairs, rows, :]
        gate_of = [
            jnp.concatenate(
                [gate_rows[:, 2 * head + b : 2 * head + b + 1] for head in range(heads)], axis=0
            )
            for b in range(2)
        ]
        scores = dot_last(
            one_sided([ready[pair, rows, :] for pair in range(pairs)], False), spans[...]
        )
        places = device * tok_rows + block * block_len + row_place
        has_span = places >= CMP - 1
        scores = jnp.where(span_ends <= places, scores * score_scale, big_negative)
        peak = jnp.max(scores, axis=-1, keepdims=True)
        raw = jnp.exp(scores - peak)
        total = jnp.where(has_span, jnp.sum(raw, axis=-1, keepdims=True), 1.0)
        summed = jnp.dot(raw.astype(jnp.bfloat16), spans[...], preferred_element_type=jnp.float32)
        mixed_spans = jnp.where(has_span, gate_of[0] * (summed[:, 64:] / total), 0.0)
        span_log = jnp.where(has_span, peak + jnp.log(total), 0.0)

        blocked = jnp.zeros(rank.shape, jnp.float32)
        for part in range(2):
            chosen_rows[part, :packed] = own[part, block]
        for number in range(named):
            source = chosen[block, number]
            z, y = source // y_count, source % y_count
            slot = z % near_count * far_count + z // near_count
            for part in range(2):
                chosen_rows[part, (number + 1) * packed : (number + 2) * packed] = arrived[
                    y, slot, part * packed : (part + 1) * packed, :
                ]
            bias = jnp.where(source < device, 0.0, big_negative)
            blocked = jnp.where(rank == number + 1, bias, blocked)
        half_scores = []
        lanes = lax.broadcasted_iota(jnp.int32, (heads * block_len, chosen_rows.shape[1]), 1)
        queries = [ready[pairs + pair, rows, :] for pair in range(pairs)]
        for upper in (False, True):
            scores = dot_last(one_sided(queries, upper), chosen_rows[0])
            scores = scores * score_scale + blocked
            later = (lanes < packed) & (lanes + packed * upper > row_place)
            half_scores.append(jnp.where(later, big_negative, scores))
        peak = jnp.maximum(
            jnp.max(half_scores[0], axis=-1, keepdims=True),
            jnp.max(half_scores[1], axis=-1, keepdims=True),
        )
        total = 0.0
        products = []
        for upper in range(2):
            raw = jnp.exp(half_scores[upper] - peak)
            total = total + jnp.sum(raw, axis=-1, keepdims=True)
            products.append(
                jnp.dot(
                    raw.astype(jnp.bfloat16), chosen_rows[1], preferred_element_type=jnp.float32
                )
            )
        summed = products[0][:, :64] + products[1][:, 64:]
        mixed = mixed_spans + gate_of[1] * (summed / total)
        chosen_log = peak + jnp.log(total)
        for pair in range(pairs):
            first = mixed[2 * pair * block_len : (2 * pair + 1) * block_len]
            second = mixed[(2 * pair + 1) * block_len : (2 * pair + 2) * block_len]
            both = jnp.concatenate([first, second], axis=1)
            lower, upper = both[:packed], both[packed:]
            lane_range = slice(pair * 128, (pair + 1) * 128)
            kept[block, :, lane_range] = jnp.where(core == 0, lower, upper).astype(jnp.bfloat16)
            given[block, :, lane_range] = jnp.where(core == 0, upper, lower).astype(jnp.bfloat16)
        for head in range(heads):
            piece = slice(head * block_len, (head + 1) * block_len)
            logs[0, rows, head : head + 1] = span_log[piece]
            logs[1, rows, head : head + 1] = chosen_log[piece]


def kernel_call(kernel, specs, operands, outputs, scratch, flops, room):
    return pl.pallas_call(
        kernel,
        out_shape=outputs,
        in_specs=[pl.BlockSpec(memory_space=space) for space in specs],
        out_specs=jax.tree.map(lambda _: pl.BlockSpec(memory_space=pltpu.VMEM), outputs),
        scratch_shapes=scratch,
        cost_estimate=pl.CostEstimate(flops=flops, bytes_accessed=4 << 20, transcendentals=0),
        compiler_params=pltpu.CompilerParams(vmem_limit_bytes=room << 20),
    )(*operands)


def turns(places, head_size):
    half_size = head_size // 2
    inverse = jnp.power(rope_base, -jnp.arange(half_size, dtype=jnp.float32) * 2.0 / head_size)
    angles = places.astype(jnp.float32)[:, None] * inverse[None, :]
    return jnp.cos(angles), jnp.sin(angles)


def shards(
    tokens,
    query_weight,
    key_weight,
    value_weight,
    gate_weight,
    query_gain,
    key_gain,
    out_weight,
    shared_block,
    chosen_device,
):
    tok_rows = tokens.shape[0]
    head_size = query_gain.shape[0]
    width = query_weight.shape[1]
    head_count = width // head_size
    packed = SEL // 2
    local_blocks = tok_rows // SEL
    device = lax.axis_index(KV)
    far_count, near_count, y_count = (lax.axis_size(axis) for axis in KV)
    z_count = far_count * near_count
    sent_rows = SEL + tok_rows // CMP
    places = device * tok_rows + jnp.arange(tok_rows, dtype=jnp.int32)
    cosines, sines = turns(places, head_size)
    bf16, f32 = jnp.bfloat16, jnp.float32
    shape = jax.ShapeDtypeStruct
    vmem, smem = pltpu.VMEM, pltpu.SMEM

    sent, own = kernel_call(
        key_kernel,
        [smem] + [vmem] * 6,
        (shared_block, tokens, key_weight.T, value_weight.T, key_gain[None], cosines, sines),
        (shape((sent_rows, 128), bf16), shape((2, local_blocks, packed, 128), bf16)),
        (),
        10**9,
        KEY_ROOM,
    )
    far = lax.all_gather(sent, "z_far", axis=0, tiled=True)
    column = lax.all_gather(far, "z_near", axis=0, tiled=True)
    arrived = spread(column, "y").reshape(y_count, z_count, sent_rows, 128)

    tokens_later, own, cosines, sines, swap_weight, _ = lax.optimization_barrier(
        (tokens, own, cosines, sines, out_weight, column)
    )
    other_weight = lax.ppermute(swap_weight, "core", [(0, 1), (1, 0)])
    ready = kernel_call(
        query_kernel,
        [smem] + [vmem] * 6,
        (
            lax.axis_index(TP).reshape(1),
            tokens_later,
            query_weight,
            gate_weight.T,
            jnp.concatenate([query_gain, query_gain])[None],
            cosines,
            sines,
        ),
        shape((2 * (width // 128) + 1, tok_rows, 128), f32),
        (),
        10**9,
        QUERY_ROOM,
    )
    kept, given, log_weight = kernel_call(
        functools.partial(attention_kernel, far_count),
        [smem, smem, vmem, vmem, vmem],
        (
            jnp.stack([device, lax.axis_index("core")]),
            chosen_device,
            arrived,
            ready,
            own,
        ),
        (
            shape((local_blocks, packed, width), bf16),
            shape((local_blocks, packed, width), bf16),
            shape((2, tok_rows, head_count), f32),
        ),
        (
            pltpu.VMEM((2, (chosen_device.shape[1] + 1) * packed, 128), bf16),
            pltpu.VMEM((y_count * z_count * (sent_rows - SEL), 128), bf16),
        ),
        4 * 10**9,
        ATTENTION_ROOM,
    )
    taken = lax.ppermute(given, "core", [(0, 1), (1, 0)])
    own_partial = jnp.dot(
        kept.reshape(-1, width), out_weight, preferred_element_type=jnp.float32
    ).astype(bf16)
    other_partial = jnp.dot(
        taken.reshape(-1, width), other_weight, preferred_element_type=jnp.float32
    ).astype(bf16)
    pair_sum = (own_partial.astype(f32) + other_partial.astype(f32)).astype(bf16)
    pair_sum = pair_sum.reshape(local_blocks, packed, -1)
    pieces = lax.all_to_all(pair_sum, "x", split_axis=0, concat_axis=0, tiled=True)
    mixed_out = pieces.astype(f32).sum(axis=0).astype(bf16)
    return (mixed_out, log_weight)


def solution(mesh):
    torus = Mesh(mesh.devices.reshape(8, 4, 4, 4, 2), (*KV, *TP))
    return jax.shard_map(
        shards,
        mesh=torus,
        in_specs=(
            P(KV, None),
            P(None, TP),
            P(None, TP),
            P(None, TP),
            P(),
            P(),
            P(),
            P(TP, None),
            P(KV),
            P(KV, None),
        ),
        out_specs=(P((*KV, *TP), None), P(None, KV, TP)),
        check_vma=False,
    )
```

```python
import functools

import jax
import jax.numpy as jnp
from jax import lax
from jax.experimental import pallas as pl
from jax.experimental.pallas import tpu as pltpu
from jax.sharding import Mesh
from jax.sharding import PartitionSpec as P

SEL = 64
CMP = 32
KV = ("z_far", "z_near", "y")
TP = ("x", "core")
KEY_ROOM = 60
QUERY_ROOM = 60
ATTENTION_ROOM = 60


norm_eps = 1e-06
rope_base = 500000.0
big_negative = -1e30


def swapped(values_in):
    half_size = values_in.shape[-1] // 2
    return jnp.concatenate([values_in[:, half_size:], values_in[:, :half_size]], axis=1)


def repeated(halves, signs):
    return jnp.concatenate([sign * halves for sign in signs], axis=1)


def side_by_side(rows):
    half_size = rows.shape[0] // 2
    return jnp.concatenate([rows[:half_size], rows[half_size:]], axis=1)


def dot_last(left, right):
    return lax.dot_general(
        left, right, (((1,), (1,)), ((), ())), preferred_element_type=jnp.float32
    )


def key_kernel(pick, tokens, key_weight, value_weight, gain, cosines, sines, sent, own):
    _, blocks, packed, _ = own.shape
    tok_rows = tokens.shape[0]
    block_len = 2 * packed
    keys = dot_last(tokens[...], key_weight[...])
    keys = keys.astype(jnp.bfloat16).astype(jnp.float32)
    values = dot_last(tokens[...], value_weight[...]).astype(jnp.bfloat16)
    square = jnp.mean(keys * keys, axis=-1, keepdims=True)
    plain = (keys * lax.rsqrt(square + norm_eps) * gain[...]).astype(jnp.bfloat16)
    plain = plain.astype(jnp.float32)
    turned = plain * repeated(cosines[...], (1, 1)) + swapped(plain) * repeated(
        sines[...], (-1, 1)
    )
    turned = turned.astype(jnp.bfloat16)
    for block in range(blocks):
        rows = slice(block * block_len, (block + 1) * block_len)
        own[0, block] = side_by_side(turned[rows])
        own[1, block] = side_by_side(values[rows])
    both = jnp.concatenate([plain, values.astype(jnp.float32)], axis=1)
    spans = jnp.mean(both.reshape(tok_rows // CMP, CMP, both.shape[1]), axis=1)
    sent[:packed] = own[0, pick[0]]
    sent[packed:block_len] = own[1, pick[0]]
    sent[block_len:] = spans.astype(jnp.bfloat16)


def query_kernel(group, tokens, query_weight, gate_weight, gain, cosines, sines, ready):
    tok_rows = tokens.shape[0]
    width = query_weight.shape[1]
    gate_count = 2 * (width // 64)
    start = pl.multiple_of(group[0] * gate_count, gate_count)
    ready[2 * (width // 128), :, :gate_count] = jax.nn.sigmoid(
        dot_last(tokens[...], gate_weight[pl.ds(start, gate_count), :].astype(jnp.bfloat16))
    )
    lanes = lax.broadcasted_iota(jnp.int32, (tok_rows, 128), 1)
    cos_lanes = repeated(cosines[...], (1, 1, 1, 1))
    sin_lanes = repeated(sines[...], (-1, 1, -1, 1))
    for pair in range(width // 128):
        queries = jnp.dot(
            tokens[...],
            query_weight[:, pair * 128 : (pair + 1) * 128],
            preferred_element_type=jnp.float32,
        )
        queries = queries.astype(jnp.bfloat16).astype(jnp.float32)
        squares = queries * queries
        first = jnp.sum(jnp.where(lanes < 64, squares, 0.0), axis=-1, keepdims=True)
        second = jnp.sum(jnp.where(lanes < 64, 0.0, squares), axis=-1, keepdims=True)
        square = jnp.where(lanes < 64, first, second) * (1.0 / 64)
        plain = (queries * lax.rsqrt(square + norm_eps) * gain[...]).astype(jnp.bfloat16)
        plain = plain.astype(jnp.float32)
        ready[pair] = plain
        partner = jnp.where(
            lanes % 64 < 32, pltpu.roll(plain, 96, axis=1), pltpu.roll(plain, 32, axis=1)
        )
        turned = plain * cos_lanes + partner * sin_lanes
        ready[width // 128 + pair] = turned.astype(jnp.bfloat16).astype(jnp.float32)


def one_sided(queries, upper):
    pieces = []
    lanes = lax.broadcasted_iota(jnp.int32, queries[0].shape, 1)
    keep = (lanes >= 64) if upper else (lanes < 64)
    for both in queries:
        turned = swapped(both)
        for piece in (turned, both) if upper else (both, turned):
            pieces.append(jnp.where(keep, piece, 0.0).astype(jnp.bfloat16))
    return jnp.concatenate(pieces, axis=0)


def attention_kernel(
    far_count,
    place_of,
    chosen,
    column_far,
    following,
    previous,
    opposite_first,
    opposite_last,
    ready_far,
    own_far,
    kept,
    given,
    logs,
    arrived,
    ready,
    own,
    chosen_rows,
    spans,
    semaphores,
):
    device, core = place_of[0], place_of[1]
    half = opposite_first.shape[0]
    loads = (
        (ready_far, ready),
        (own_far, own),
        (column_far, arrived.at[0]),
        (following, arrived.at[1]),
        (opposite_first, arrived.at[2, :half]),
        (opposite_last, arrived.at[2, half:]),
        (previous, arrived.at[3]),
    )
    loads = [
        pltpu.make_async_copy(source, target, semaphores.at[number])
        for number, (source, target) in enumerate(loads)
    ]
    for load in loads:
        load.start()
    for load in loads:
        load.wait()
    blocks, named = chosen.shape
    _, _, packed, _ = own.shape
    y_count, z_count, sent_rows, _ = arrived.shape
    block_len = 2 * packed
    pairs = kept.shape[2] // 128
    heads = 2 * pairs
    tok_rows = blocks * block_len
    span_rows = sent_rows - block_len
    score_scale = 64 ** (-0.5)
    column_rows = z_count * span_rows
    for y in range(y_count):
        column = arrived[y, :, block_len:, :].astype(jnp.float32)
        spans[y * column_rows : (y + 1) * column_rows] = column.reshape(column_rows, 128).astype(
            jnp.bfloat16
        )
    row_place = lax.broadcasted_iota(jnp.int32, (heads * block_len, 1), 0) % block_len
    span_index = lax.broadcasted_iota(jnp.int32, (1, y_count * column_rows), 1)
    slot = span_index % column_rows // span_rows
    near_count = z_count // far_count
    owner = (slot % far_count * near_count + slot // far_count) * y_count
    owner = owner + (device % y_count + span_index // column_rows) % y_count
    span_ends = owner * tok_rows + span_index % span_rows * CMP + CMP - 1
    rank = lax.broadcasted_iota(jnp.int32, (1, chosen_rows.shape[1]), 1) // packed

    @pl.loop(0, blocks)
    def _(block):
        rows = pl.ds(pl.multiple_of(block * block_len, block_len), block_len)
        gate_rows = ready[2 * pairs, rows, :]
        gate_of = [
            jnp.concatenate(
                [gate_rows[:, 2 * head + b : 2 * head + b + 1] for head in range(heads)], axis=0
            )
            for b in range(2)
        ]
        scores = dot_last(
            one_sided([ready[pair, rows, :] for pair in range(pairs)], False), spans[...]
        )
        places = device * tok_rows + block * block_len + row_place
        has_span = places >= CMP - 1
        scores = jnp.where(span_ends <= places, scores * score_scale, big_negative)
        peak = jnp.max(scores, axis=-1, keepdims=True)
        raw = jnp.exp(scores - peak)
        total = jnp.where(has_span, jnp.sum(raw, axis=-1, keepdims=True), 1.0)
        summed = jnp.dot(raw.astype(jnp.bfloat16), spans[...], preferred_element_type=jnp.float32)
        mixed_spans = jnp.where(has_span, gate_of[0] * (summed[:, 64:] / total), 0.0)
        span_log = jnp.where(has_span, peak + jnp.log(total), 0.0)

        blocked = jnp.zeros(rank.shape, jnp.float32)
        for part in range(2):
            chosen_rows[part, :packed] = own[part, block]
        for number in range(named):
            source = chosen[block, number]
            z, y = source // y_count, (source + y_count - device % y_count) % y_count
            slot = z % near_count * far_count + z // near_count
            for part in range(2):
                chosen_rows[part, (number + 1) * packed : (number + 2) * packed] = arrived[
                    y, slot, part * packed : (part + 1) * packed, :
                ]
            bias = jnp.where(source < device, 0.0, big_negative)
            blocked = jnp.where(rank == number + 1, bias, blocked)
        half_scores = []
        lanes = lax.broadcasted_iota(jnp.int32, (heads * block_len, chosen_rows.shape[1]), 1)
        queries = [ready[pairs + pair, rows, :] for pair in range(pairs)]
        for upper in (False, True):
            scores = dot_last(one_sided(queries, upper), chosen_rows[0])
            scores = scores * score_scale + blocked
            later = (lanes < packed) & (lanes + packed * upper > row_place)
            half_scores.append(jnp.where(later, big_negative, scores))
        peak = jnp.maximum(
            jnp.max(half_scores[0], axis=-1, keepdims=True),
            jnp.max(half_scores[1], axis=-1, keepdims=True),
        )
        total = 0.0
        products = []
        for upper in range(2):
            raw = jnp.exp(half_scores[upper] - peak)
            total = total + jnp.sum(raw, axis=-1, keepdims=True)
            products.append(
                jnp.dot(
                    raw.astype(jnp.bfloat16), chosen_rows[1], preferred_element_type=jnp.float32
                )
            )
        summed = products[0][:, :64] + products[1][:, 64:]
        mixed = mixed_spans + gate_of[1] * (summed / total)
        chosen_log = peak + jnp.log(total)
        for pair in range(pairs):
            first = mixed[2 * pair * block_len : (2 * pair + 1) * block_len]
            second = mixed[(2 * pair + 1) * block_len : (2 * pair + 2) * block_len]
            both = jnp.concatenate([first, second], axis=1)
            lower, upper = both[:packed], both[packed:]
            lane_range = slice(pair * 128, (pair + 1) * 128)
            kept[block, :, lane_range] = jnp.where(core == 0, lower, upper).astype(jnp.bfloat16)
            given[block, :, lane_range] = jnp.where(core == 0, upper, lower).astype(jnp.bfloat16)
        for head in range(heads):
            piece = slice(head * block_len, (head + 1) * block_len)
            logs[0, rows, head : head + 1] = span_log[piece]
            logs[1, rows, head : head + 1] = chosen_log[piece]


def kernel_call(kernel, specs, operands, outputs, scratch, flops, room):
    return pl.pallas_call(
        kernel,
        out_shape=outputs,
        in_specs=[pl.BlockSpec(memory_space=space) for space in specs],
        out_specs=jax.tree.map(lambda _: pl.BlockSpec(memory_space=pltpu.VMEM), outputs),
        scratch_shapes=scratch,
        cost_estimate=pl.CostEstimate(flops=flops, bytes_accessed=4 << 20, transcendentals=0),
        compiler_params=pltpu.CompilerParams(vmem_limit_bytes=room << 20),
    )(*operands)


def turns(places, head_size):
    half_size = head_size // 2
    inverse = jnp.power(rope_base, -jnp.arange(half_size, dtype=jnp.float32) * 2.0 / head_size)
    angles = places.astype(jnp.float32)[:, None] * inverse[None, :]
    return jnp.cos(angles), jnp.sin(angles)


def shards(
    tokens,
    query_weight,
    key_weight,
    value_weight,
    gate_weight,
    query_gain,
    key_gain,
    out_weight,
    shared_block,
    chosen_device,
):
    tok_rows = tokens.shape[0]
    head_size = query_gain.shape[0]
    width = query_weight.shape[1]
    head_count = width // head_size
    packed = SEL // 2
    local_blocks = tok_rows // SEL
    device = lax.axis_index(KV)
    far_count, near_count, y_count = (lax.axis_size(axis) for axis in KV)
    z_count = far_count * near_count
    sent_rows = SEL + tok_rows // CMP
    places = device * tok_rows + jnp.arange(tok_rows, dtype=jnp.int32)
    cosines, sines = turns(places, head_size)
    bf16, f32 = jnp.bfloat16, jnp.float32
    shape = jax.ShapeDtypeStruct
    vmem, smem = pltpu.VMEM, pltpu.SMEM

    sent, own = kernel_call(
        key_kernel,
        [smem] + [vmem] * 6,
        (shared_block, tokens, key_weight.T, value_weight.T, key_gain[None], cosines, sines),
        (shape((sent_rows, 128), bf16), shape((2, local_blocks, packed, 128), bf16)),
        (),
        10**9,
        KEY_ROOM,
    )
    far = lax.all_gather(sent, "z_far", axis=0, tiled=True)
    column = lax.all_gather(far, "z_near", axis=0, tiled=True)
    ahead = [(place, (place + 1) % y_count) for place in range(y_count)]
    back = [(place, (place - 1) % y_count) for place in range(y_count)]
    half_rows = column.shape[0] // 2
    previous = lax.ppermute(column, "y", ahead)
    following = lax.ppermute(column, "y", back)
    opposite_first = lax.ppermute(previous[:half_rows], "y", ahead)
    opposite_last = lax.ppermute(following[half_rows:], "y", back)
    pieces = [
        piece.reshape(-1, sent_rows, 128)
        for piece in (column, following, previous, opposite_first, opposite_last)
    ]

    tokens_later, swap_weight, own, cosines, sines, _ = lax.optimization_barrier(
        (tokens, out_weight, own, cosines, sines, column)
    )
    ready = kernel_call(
        query_kernel,
        [smem] + [vmem] * 6,
        (
            lax.axis_index(TP).reshape(1),
            tokens_later,
            query_weight,
            gate_weight.T,
            jnp.concatenate([query_gain, query_gain])[None],
            cosines,
            sines,
        ),
        shape((2 * (width // 128) + 1, tok_rows, 128), f32),
        (),
        10**9,
        QUERY_ROOM,
    )
    other_weight = lax.ppermute(swap_weight, "core", [(0, 1), (1, 0)])
    kept, given, log_weight = kernel_call(
        functools.partial(attention_kernel, far_count),
        [smem, smem] + [pl.ANY] * 7,
        (
            jnp.stack([device, lax.axis_index("core")]),
            chosen_device,
            *pieces,
            ready,
            own,
        ),
        (
            shape((local_blocks, packed, width), bf16),
            shape((local_blocks, packed, width), bf16),
            shape((2, tok_rows, head_count), f32),
        ),
        (
            pltpu.VMEM((y_count, z_count, sent_rows, 128), bf16),
            pltpu.VMEM(ready.shape, f32),
            pltpu.VMEM(own.shape, bf16),
            pltpu.VMEM((2, (chosen_device.shape[1] + 1) * packed, 128), bf16),
            pltpu.VMEM((y_count * z_count * (sent_rows - SEL), 128), bf16),
            pltpu.SemaphoreType.DMA((7,)),
        ),
        4 * 10**9,
        ATTENTION_ROOM,
    )
    taken = lax.ppermute(given, "core", [(0, 1), (1, 0)])
    own_partial = jnp.dot(
        kept.reshape(-1, width), out_weight, preferred_element_type=jnp.float32
    ).astype(bf16)
    other_partial = jnp.dot(
        taken.reshape(-1, width), other_weight, preferred_element_type=jnp.float32
    ).astype(bf16)
    pair_sum = (own_partial.astype(f32) + other_partial.astype(f32)).astype(bf16)
    pair_sum = pair_sum.reshape(local_blocks, packed, -1)
    partials = lax.all_to_all(pair_sum, "x", split_axis=0, concat_axis=0, tiled=True)
    mixed_out = partials.astype(f32).sum(axis=0).astype(bf16)
    return (mixed_out, log_weight)


def solution(mesh):
    torus = Mesh(mesh.devices.reshape(8, 4, 4, 4, 2), (*KV, *TP))
    return jax.shard_map(
        shards,
        mesh=torus,
        in_specs=(
            P(KV, None),
            P(None, TP),
            P(None, TP),
            P(None, TP),
            P(),
            P(),
            P(),
            P(TP, None),
            P(KV),
            P(KV, None),
        ),
        out_specs=(P((*KV, *TP), None), P(None, KV, TP)),
        check_vma=False,
    )
```

```python
import functools

import jax
import jax.numpy as jnp
import numpy as np
from jax import lax
from jax.experimental import pallas as pl
from jax.experimental.pallas import tpu as pltpu
from jax.sharding import Mesh
from jax.sharding import PartitionSpec as P

SEL = 64
CMP = 32
KV = ("z_far", "z_near", "y")
TP = ("x", "core")
KEY_ROOM = 60
QUERY_ROOM = 60
ATTENTION_ROOM = 12


norm_eps = 1e-06
rope_base = 500000.0
big_negative = -1e30


def spread(block, axis):
    count = lax.axis_size(axis)
    copies = lax.optimization_barrier(jnp.broadcast_to(block[None], (count, *block.shape)))
    return lax.all_to_all(copies, axis, split_axis=0, concat_axis=0, tiled=True)


def swapped(values_in):
    half_size = values_in.shape[-1] // 2
    return jnp.concatenate([values_in[:, half_size:], values_in[:, :half_size]], axis=1)


def repeated(halves, signs):
    return jnp.concatenate([sign * halves for sign in signs], axis=1)


def side_by_side(rows):
    half_size = rows.shape[0] // 2
    return jnp.concatenate([rows[:half_size], rows[half_size:]], axis=1)


def dot_last(left, right):
    return lax.dot_general(
        left, right, (((1,), (1,)), ((), ())), preferred_element_type=jnp.float32
    )


def turns_of(start, within):
    cosines = start[0:1] * within[0] - start[1:2] * within[1]
    sines = start[1:2] * within[0] + start[0:1] * within[1]
    return cosines, sines


def key_kernel(pick, tokens, key_weight, value_weight, gain, start, within, sent, own):
    _, blocks, packed, _ = own.shape
    tok_rows = tokens.shape[0]
    block_len = 2 * packed
    keys = dot_last(tokens[...], key_weight[...])
    keys = keys.astype(jnp.bfloat16).astype(jnp.float32)
    values = dot_last(tokens[...], value_weight[...]).astype(jnp.bfloat16)
    square = jnp.mean(keys * keys, axis=-1, keepdims=True)
    plain = (keys * lax.rsqrt(square + norm_eps) * gain[...]).astype(jnp.bfloat16)
    plain = plain.astype(jnp.float32)
    cosines, sines = turns_of(start[...], within[...])
    turned = plain * repeated(cosines, (1, 1)) + swapped(plain) * repeated(sines, (-1, 1))
    turned = turned.astype(jnp.bfloat16)
    for block in range(blocks):
        rows = slice(block * block_len, (block + 1) * block_len)
        own[0, block] = side_by_side(turned[rows])
        own[1, block] = side_by_side(values[rows])
    both = jnp.concatenate([plain, values.astype(jnp.float32)], axis=1)
    spans = jnp.mean(both.reshape(tok_rows // CMP, CMP, both.shape[1]), axis=1)
    sent[:packed] = own[0, pick[0]]
    sent[packed:block_len] = own[1, pick[0]]
    sent[block_len:] = spans.astype(jnp.bfloat16)


def query_kernel(group, tokens, query_weight, gate_weight, gain, turn_start, within, ready):
    tok_rows = tokens.shape[0]
    width = query_weight.shape[1]
    gate_count = 2 * (width // 64)
    start = pl.multiple_of(group[0] * gate_count, gate_count)
    ready[2 * (width // 128), :, :gate_count] = jax.nn.sigmoid(
        dot_last(tokens[...], gate_weight[pl.ds(start, gate_count), :].astype(jnp.bfloat16))
    )
    lanes = lax.broadcasted_iota(jnp.int32, (tok_rows, 128), 1)
    cosines, sines = turns_of(turn_start[...], within[...])
    cos_lanes = repeated(cosines, (1, 1, 1, 1))
    sin_lanes = repeated(sines, (-1, 1, -1, 1))
    for pair in range(width // 128):
        queries = jnp.dot(
            tokens[...],
            query_weight[:, pair * 128 : (pair + 1) * 128],
            preferred_element_type=jnp.float32,
        )
        queries = queries.astype(jnp.bfloat16).astype(jnp.float32)
        squares = queries * queries
        first = jnp.sum(jnp.where(lanes < 64, squares, 0.0), axis=-1, keepdims=True)
        second = jnp.sum(jnp.where(lanes < 64, 0.0, squares), axis=-1, keepdims=True)
        square = jnp.where(lanes < 64, first, second) * (1.0 / 64)
        plain = (queries * lax.rsqrt(square + norm_eps) * gain[...]).astype(jnp.bfloat16)
        plain = plain.astype(jnp.float32)
        ready[pair] = plain
        partner = jnp.where(
            lanes % 64 < 32, pltpu.roll(plain, 96, axis=1), pltpu.roll(plain, 32, axis=1)
        )
        turned = plain * cos_lanes + partner * sin_lanes
        ready[width // 128 + pair] = turned.astype(jnp.bfloat16).astype(jnp.float32)


def one_sided(queries, upper):
    pieces = []
    lanes = lax.broadcasted_iota(jnp.int32, queries[0].shape, 1)
    keep = (lanes >= 64) if upper else (lanes < 64)
    for both in queries:
        turned = swapped(both)
        for piece in (turned, both) if upper else (both, turned):
            pieces.append(jnp.where(keep, piece, 0.0).astype(jnp.bfloat16))
    return jnp.concatenate(pieces, axis=0)


def attention_kernel(
    far_count,
    place_of,
    chosen,
    arrived,
    ready,
    own,
    kept,
    given,
    logs,
    chosen_rows,
    spans,
    span_part,
    span_log,
):
    device, core = place_of[0], place_of[1]
    blocks, named = chosen.shape
    _, _, packed, _ = own.shape
    y_count, z_count, sent_rows, _ = arrived.shape
    block_len = 2 * packed
    pairs = kept.shape[2] // 128
    heads = 2 * pairs
    tok_rows = blocks * block_len
    span_rows = sent_rows - block_len
    near_count = z_count // far_count
    score_scale = 64 ** (-0.5)
    all_spans = spans.shape[0]
    all_rows = chosen_rows.shape[1]

    def slot_of(z):
        return z % near_count * far_count + z // near_count

    for z in range(z_count):
        plane = jnp.concatenate(
            [
                arrived[y, slot_of(z), block_len:, :].astype(jnp.float32)
                for y in range(y_count)
            ],
            axis=0,
        )
        spans[z * y_count * span_rows : (z + 1) * y_count * span_rows] = plane.astype(jnp.bfloat16)
    chosen_rows[...] = jnp.zeros_like(chosen_rows)
    row_place = lax.broadcasted_iota(jnp.int32, (heads * block_len, 1), 0) % block_len

    def in_width(count, widths, branch):
        least = 0
        for width, most in widths:

            @pl.when((count >= least) & (count < most))
            def _():
                branch(width)

            least = most

    @pl.loop(0, blocks)
    def _(block):
        rows = pl.ds(pl.multiple_of(block * block_len, block_len), block_len)
        gate_rows = ready[2 * pairs, rows, :]
        gate_of = [
            jnp.concatenate(
                [gate_rows[:, 2 * head + b : 2 * head + b + 1] for head in range(heads)], axis=0
            )
            for b in range(2)
        ]

        def span_branch(width):
            scores = dot_last(
                one_sided([ready[pair, rows, :] for pair in range(pairs)], False), spans[:width]
            )
            places = device * tok_rows + block * block_len + row_place
            has_span = places >= CMP - 1
            span_ends = lax.broadcasted_iota(jnp.int32, (1, width), 1) * CMP + CMP - 1
            scores = jnp.where(span_ends <= places, scores * score_scale, big_negative)
            peak = jnp.max(scores, axis=-1, keepdims=True)
            raw = jnp.exp(scores - peak)
            total = jnp.where(has_span, jnp.sum(raw, axis=-1, keepdims=True), 1.0)
            summed = jnp.dot(
                raw.astype(jnp.bfloat16), spans[:width], preferred_element_type=jnp.float32
            )
            span_part[...] = jnp.where(has_span, gate_of[0] * (summed[:, 64:] / total), 0.0)
            span_log[...] = jnp.where(has_span, peak + jnp.log(total), 0.0)

        in_width(
            (device + 1) * span_rows - 1,
            [(width, width) for width in (all_spans // 4, all_spans // 2, all_spans)],
            span_branch,
        )

        for part in range(2):
            chosen_rows[part, :packed] = own[part, block]
        counted = jnp.int32(1)
        for number in range(named):
            source = chosen[block, number]
            start = pl.multiple_of(counted * packed, packed)

            @pl.when(source < device)
            def _():
                for part in range(2):
                    chosen_rows[part, pl.ds(start, packed)] = arrived[
                        source % y_count,
                        slot_of(source // y_count),
                        part * packed : (part + 1) * packed,
                        :,
                    ]

            counted = counted + jnp.where(source < device, 1, 0)
        queries = [ready[pairs + pair, rows, :] for pair in range(pairs)]

        def chosen_branch(width):
            half_scores = []
            lanes = lax.broadcasted_iota(jnp.int32, (heads * block_len, width), 1)
            blocked = jnp.where(lanes[:1] < counted * packed, 0.0, big_negative)
            for upper in (False, True):
                scores = dot_last(one_sided(queries, upper), chosen_rows[0, :width])
                scores = scores * score_scale + blocked
                later = (lanes < packed) & (lanes + packed * upper > row_place)
                half_scores.append(jnp.where(later, big_negative, scores))
            peak = jnp.maximum(
                jnp.max(half_scores[0], axis=-1, keepdims=True),
                jnp.max(half_scores[1], axis=-1, keepdims=True),
            )
            total = 0.0
            products = []
            for upper in range(2):
                raw = jnp.exp(half_scores[upper] - peak)
                total = total + jnp.sum(raw, axis=-1, keepdims=True)
                products.append(
                    jnp.dot(
                        raw.astype(jnp.bfloat16),
                        chosen_rows[1, :width],
                        preferred_element_type=jnp.float32,
                    )
                )
            summed = products[0][:, :64] + products[1][:, 64:]
            mixed = span_part[...] + gate_of[1] * (summed / total)
            chosen_log = peak + jnp.log(total)
            for pair in range(pairs):
                first = mixed[2 * pair * block_len : (2 * pair + 1) * block_len]
                second = mixed[(2 * pair + 1) * block_len : (2 * pair + 2) * block_len]
                both = jnp.concatenate([first, second], axis=1)
                lower, upper = both[:packed], both[packed:]
                lane_range = slice(pair * 128, (pair + 1) * 128)
                kept[block, :, lane_range] = jnp.where(core == 0, lower, upper).astype(
                    jnp.bfloat16
                )
                given[block, :, lane_range] = jnp.where(core == 0, upper, lower).astype(
                    jnp.bfloat16
                )
            for head in range(heads):
                piece = slice(head * block_len, (head + 1) * block_len)
                logs[0, rows, head : head + 1] = span_log[piece]
                logs[1, rows, head : head + 1] = chosen_log[piece]

        in_width(
            counted - 1,
            [(width, width // packed) for width in (all_rows // 4, all_rows // 2, all_rows)],
            chosen_branch,
        )


def kernel_call(kernel, specs, operands, outputs, scratch, flops, room):
    return pl.pallas_call(
        kernel,
        out_shape=outputs,
        in_specs=[pl.BlockSpec(memory_space=space) for space in specs],
        out_specs=jax.tree.map(lambda _: pl.BlockSpec(memory_space=pltpu.VMEM), outputs),
        scratch_shapes=scratch,
        cost_estimate=pl.CostEstimate(flops=flops, bytes_accessed=4 << 20, transcendentals=0),
        compiler_params=pltpu.CompilerParams(vmem_limit_bytes=room << 20),
    )(*operands)


def turns(first_place, tok_rows, head_size):
    half_size = head_size // 2
    exact = rope_base ** (-np.arange(half_size) * 2.0 / head_size)
    within = np.arange(tok_rows)[:, None] * exact[None, :]
    start = first_place.astype(jnp.float32) * exact.astype(np.float32)
    return (
        jnp.stack([jnp.cos(start), jnp.sin(start)]),
        jnp.asarray(np.stack([np.cos(within), np.sin(within)]).astype(np.float32)),
    )


def shards(
    tokens,
    query_weight,
    key_weight,
    value_weight,
    gate_weight,
    query_gain,
    key_gain,
    out_weight,
    shared_block,
    chosen_device,
):
    tok_rows = tokens.shape[0]
    head_size = query_gain.shape[0]
    width = query_weight.shape[1]
    head_count = width // head_size
    packed = SEL // 2
    local_blocks = tok_rows // SEL
    device = lax.axis_index(KV)
    far_count, near_count, y_count = (lax.axis_size(axis) for axis in KV)
    z_count = far_count * near_count
    sent_rows = SEL + tok_rows // CMP
    turn_start, within = turns(device * tok_rows, tok_rows, head_size)
    bf16, f32 = jnp.bfloat16, jnp.float32
    shape = jax.ShapeDtypeStruct
    vmem, smem = pltpu.VMEM, pltpu.SMEM

    sent, own = kernel_call(
        key_kernel,
        [smem] + [vmem] * 6,
        (shared_block, tokens, key_weight.T, value_weight.T, key_gain[None], turn_start, within),
        (shape((sent_rows, 128), bf16), shape((2, local_blocks, packed, 128), bf16)),
        (),
        10**9,
        KEY_ROOM,
    )
    far = lax.all_gather(sent, "z_far", axis=0, tiled=True)
    column = lax.all_gather(far, "z_near", axis=0, tiled=True)
    arrived = spread(column, "y").reshape(y_count, z_count, sent_rows, 128)

    tokens_later, own, turn_start, swap_weight, _ = lax.optimization_barrier(
        (tokens, own, turn_start, out_weight, column)
    )
    other_weight = lax.ppermute(swap_weight, "core", [(0, 1), (1, 0)])
    ready = kernel_call(
        query_kernel,
        [smem] + [vmem] * 6,
        (
            lax.axis_index(TP).reshape(1),
            tokens_later,
            query_weight,
            gate_weight.T,
            jnp.concatenate([query_gain, query_gain])[None],
            turn_start,
            within,
        ),
        shape((2 * (width // 128) + 1, tok_rows, 128), f32),
        (),
        10**9,
        QUERY_ROOM,
    )
    kept, given, log_weight = kernel_call(
        functools.partial(attention_kernel, far_count),
        [smem, smem, vmem, vmem, vmem],
        (
            jnp.stack([device, lax.axis_index("core")]),
            chosen_device,
            arrived,
            ready,
            own,
        ),
        (
            shape((local_blocks, packed, width), bf16),
            shape((local_blocks, packed, width), bf16),
            shape((2, tok_rows, head_count), f32),
        ),
        (
            pltpu.VMEM((2, (chosen_device.shape[1] + 1) * packed, 128), bf16),
            pltpu.VMEM((y_count * z_count * (sent_rows - SEL), 128), bf16),
            pltpu.VMEM((head_count * SEL, head_size), f32),
            pltpu.VMEM((head_count * SEL, 1), f32),
        ),
        4 * 10**9,
        ATTENTION_ROOM,
    )
    taken = lax.ppermute(given, "core", [(0, 1), (1, 0)])
    own_partial = jnp.dot(
        kept.reshape(-1, width), out_weight, preferred_element_type=jnp.float32
    ).astype(bf16)
    other_partial = jnp.dot(
        taken.reshape(-1, width), other_weight, preferred_element_type=jnp.float32
    ).astype(bf16)
    pair_sum = (own_partial.astype(f32) + other_partial.astype(f32)).astype(bf16)
    pair_sum = pair_sum.reshape(local_blocks, packed, -1)
    pieces = lax.all_to_all(pair_sum, "x", split_axis=0, concat_axis=0, tiled=True)
    mixed_out = pieces.astype(f32).sum(axis=0).astype(bf16)
    return (mixed_out, log_weight)


def solution(mesh):
    torus = Mesh(mesh.devices.reshape(8, 4, 4, 4, 2), (*KV, *TP))
    return jax.shard_map(
        shards,
        mesh=torus,
        in_specs=(
            P(KV, None),
            P(None, TP),
            P(None, TP),
            P(None, TP),
            P(),
            P(),
            P(),
            P(TP, None),
            P(KV),
            P(KV, None),
        ),
        out_specs=(P((*KV, *TP), None), P(None, KV, TP)),
        check_vma=False,
    )
```

```python
import functools

import jax
import jax.numpy as jnp
import numpy as np
from jax import lax
from jax.experimental import pallas as pl
from jax.experimental.pallas import tpu as pltpu
from jax.sharding import Mesh
from jax.sharding import PartitionSpec as P

SEL = 64
CMP = 32
KV = ("z_far", "z_near", "y")
TP = ("x", "core")
KEY_ROOM = 60
QUERY_ROOM = 60
ATTENTION_ROOM = 12


norm_eps = 1e-06
rope_base = 500000.0
big_negative = -1e30


def spread(block, axis):
    count = lax.axis_size(axis)
    copies = lax.optimization_barrier(jnp.broadcast_to(block[None], (count, *block.shape)))
    return lax.all_to_all(copies, axis, split_axis=0, concat_axis=0, tiled=True)


def swapped(values_in):
    half_size = values_in.shape[-1] // 2
    return jnp.concatenate([values_in[:, half_size:], values_in[:, :half_size]], axis=1)


def repeated(halves, signs):
    return jnp.concatenate([sign * halves for sign in signs], axis=1)


def side_by_side(rows):
    half_size = rows.shape[0] // 2
    return jnp.concatenate([rows[:half_size], rows[half_size:]], axis=1)


def dot_last(left, right):
    return lax.dot_general(
        left, right, (((1,), (1,)), ((), ())), preferred_element_type=jnp.float32
    )


def turns_of(start_cosines, start_sines, within):
    cosines = start_cosines * within[0] - start_sines * within[1]
    sines = start_sines * within[0] + start_cosines * within[1]
    return cosines, sines


def key_kernel(pick, tokens, key_weight, value_weight, gain, start_cosines, start_sines, within, sent, own):
    _, blocks, packed, _ = own.shape
    tok_rows = tokens.shape[0]
    block_len = 2 * packed
    keys = dot_last(tokens[...], key_weight[...])
    keys = keys.astype(jnp.bfloat16).astype(jnp.float32)
    values = dot_last(tokens[...], value_weight[...]).astype(jnp.bfloat16)
    square = jnp.mean(keys * keys, axis=-1, keepdims=True)
    plain = (keys * lax.rsqrt(square + norm_eps) * gain[...]).astype(jnp.bfloat16)
    plain = plain.astype(jnp.float32)
    cosines, sines = turns_of(start_cosines[...], start_sines[...], within[...])
    turned = plain * repeated(cosines, (1, 1)) + swapped(plain) * repeated(sines, (-1, 1))
    turned = turned.astype(jnp.bfloat16)
    for block in range(blocks):
        rows = slice(block * block_len, (block + 1) * block_len)
        own[0, block] = side_by_side(turned[rows])
        own[1, block] = side_by_side(values[rows])
    both = jnp.concatenate([plain, values.astype(jnp.float32)], axis=1)
    spans = jnp.mean(both.reshape(tok_rows // CMP, CMP, both.shape[1]), axis=1)
    sent[:packed] = own[0, pick[0]]
    sent[packed:block_len] = own[1, pick[0]]
    sent[block_len:] = spans.astype(jnp.bfloat16)


def query_kernel(group, tokens, query_weight, gate_weight, gain, start_cosines, start_sines, within, ready):
    tok_rows = tokens.shape[0]
    width = query_weight.shape[1]
    gate_count = 2 * (width // 64)
    start = pl.multiple_of(group[0] * gate_count, gate_count)
    ready[2 * (width // 128), :, :gate_count] = jax.nn.sigmoid(
        dot_last(tokens[...], gate_weight[pl.ds(start, gate_count), :].astype(jnp.bfloat16))
    )
    lanes = lax.broadcasted_iota(jnp.int32, (tok_rows, 128), 1)
    cosines, sines = turns_of(start_cosines[...], start_sines[...], within[...])
    cos_lanes = repeated(cosines, (1, 1, 1, 1))
    sin_lanes = repeated(sines, (-1, 1, -1, 1))
    for pair in range(width // 128):
        queries = jnp.dot(
            tokens[...],
            query_weight[:, pair * 128 : (pair + 1) * 128],
            preferred_element_type=jnp.float32,
        )
        queries = queries.astype(jnp.bfloat16).astype(jnp.float32)
        squares = queries * queries
        first = jnp.sum(jnp.where(lanes < 64, squares, 0.0), axis=-1, keepdims=True)
        second = jnp.sum(jnp.where(lanes < 64, 0.0, squares), axis=-1, keepdims=True)
        square = jnp.where(lanes < 64, first, second) * (1.0 / 64)
        plain = (queries * lax.rsqrt(square + norm_eps) * gain[...]).astype(jnp.bfloat16)
        plain = plain.astype(jnp.float32)
        ready[pair] = plain
        partner = jnp.where(
            lanes % 64 < 32, pltpu.roll(plain, 96, axis=1), pltpu.roll(plain, 32, axis=1)
        )
        turned = plain * cos_lanes + partner * sin_lanes
        ready[width // 128 + pair] = turned.astype(jnp.bfloat16).astype(jnp.float32)


def one_sided(queries, upper):
    pieces = []
    lanes = lax.broadcasted_iota(jnp.int32, queries[0].shape, 1)
    keep = (lanes >= 64) if upper else (lanes < 64)
    for both in queries:
        turned = swapped(both)
        for piece in (turned, both) if upper else (both, turned):
            pieces.append(jnp.where(keep, piece, 0.0).astype(jnp.bfloat16))
    return jnp.concatenate(pieces, axis=0)


def attention_kernel(
    far_count,
    place_of,
    chosen,
    arrived,
    ready,
    own,
    kept,
    given,
    logs,
    chosen_rows,
    spans,
    span_part,
    span_log,
):
    device, core = place_of[0], place_of[1]
    blocks, named = chosen.shape
    _, _, packed, _ = own.shape
    y_count, z_count, sent_rows, _ = arrived.shape
    block_len = 2 * packed
    pairs = kept.shape[2] // 128
    heads = 2 * pairs
    tok_rows = blocks * block_len
    span_rows = sent_rows - block_len
    near_count = z_count // far_count
    score_scale = 64 ** (-0.5)
    all_spans = spans.shape[0]
    all_rows = chosen_rows.shape[1]

    near_bits, y_bits = near_count.bit_length() - 1, y_count.bit_length() - 1

    def slot_of(z):
        return (z & (near_count - 1)) * far_count + (z >> near_bits)

    plane_rows = y_count * span_rows
    for first in range(0, z_count, far_count):

        @pl.when(first << y_bits <= device)
        def _():
            for z in range(first, first + far_count):
                plane = jnp.concatenate(
                    [
                        arrived[y, slot_of(z), block_len:, :].astype(jnp.float32)
                        for y in range(y_count)
                    ],
                    axis=0,
                )
                spans[z * plane_rows : (z + 1) * plane_rows] = plane.astype(jnp.bfloat16)

        @pl.when(first << y_bits > device)
        def _():
            rows = slice(first * plane_rows, (first + far_count) * plane_rows)
            spans[rows] = jnp.zeros((far_count * plane_rows, 128), jnp.bfloat16)

    chosen_rows[...] = jnp.zeros_like(chosen_rows)
    row_place = lax.broadcasted_iota(jnp.int32, (heads * block_len, 1), 0) % block_len

    def in_width(count, widths, branch):
        least = 0
        for width, most in widths:

            @pl.when((count >= least) & (count < most))
            def _():
                branch(width)

            least = most

    @pl.loop(0, blocks)
    def _(block):
        rows = pl.ds(pl.multiple_of(block * block_len, block_len), block_len)
        gate_rows = ready[2 * pairs, rows, :]
        gate_of = [
            jnp.concatenate(
                [gate_rows[:, 2 * head + b : 2 * head + b + 1] for head in range(heads)], axis=0
            )
            for b in range(2)
        ]

        def span_branch(width):
            scores = dot_last(
                one_sided([ready[pair, rows, :] for pair in range(pairs)], False), spans[:width]
            )
            places = device * tok_rows + block * block_len + row_place
            has_span = places >= CMP - 1
            span_ends = lax.broadcasted_iota(jnp.int32, (1, width), 1) * CMP + CMP - 1
            scores = jnp.where(span_ends <= places, scores * score_scale, big_negative)
            peak = jnp.max(scores, axis=-1, keepdims=True)
            raw = jnp.exp(scores - peak)
            total = jnp.where(has_span, jnp.sum(raw, axis=-1, keepdims=True), 1.0)
            summed = jnp.dot(
                raw.astype(jnp.bfloat16), spans[:width], preferred_element_type=jnp.float32
            )
            span_part[...] = jnp.where(has_span, gate_of[0] * (summed[:, 64:] / total), 0.0)
            span_log[...] = jnp.where(has_span, peak + jnp.log(total), 0.0)

        in_width(
            (device + 1) * span_rows - 1,
            [(width, width) for width in (all_spans // 4, all_spans // 2, all_spans)],
            span_branch,
        )

        for part in range(2):
            chosen_rows[part, :packed] = own[part, block]
        counted = jnp.int32(1)
        for number in range(named):
            source = chosen[block, number]
            start = pl.multiple_of(counted * packed, packed)
            y, slot = source & (y_count - 1), slot_of(source >> y_bits)
            for part in range(2):
                chosen_rows[part, pl.ds(start, packed)] = arrived[
                    y, slot, part * packed : (part + 1) * packed, :
                ]
            counted = counted + jnp.where(source < device, 1, 0)
        queries = [ready[pairs + pair, rows, :] for pair in range(pairs)]

        def chosen_branch(width):
            half_scores = []
            lanes = lax.broadcasted_iota(jnp.int32, (heads * block_len, width), 1)
            blocked = jnp.where(lanes[:1] < counted * packed, 0.0, big_negative)
            for upper in (False, True):
                scores = dot_last(one_sided(queries, upper), chosen_rows[0, :width])
                scores = scores * score_scale + blocked
                later = (lanes < packed) & (lanes + packed * upper > row_place)
                half_scores.append(jnp.where(later, big_negative, scores))
            peak = jnp.maximum(
                jnp.max(half_scores[0], axis=-1, keepdims=True),
                jnp.max(half_scores[1], axis=-1, keepdims=True),
            )
            total = 0.0
            products = []
            for upper in range(2):
                raw = jnp.exp(half_scores[upper] - peak)
                total = total + jnp.sum(raw, axis=-1, keepdims=True)
                products.append(
                    jnp.dot(
                        raw.astype(jnp.bfloat16),
                        chosen_rows[1, :width],
                        preferred_element_type=jnp.float32,
                    )
                )
            summed = products[0][:, :64] + products[1][:, 64:]
            mixed = span_part[...] + gate_of[1] * (summed / total)
            chosen_log = peak + jnp.log(total)
            for pair in range(pairs):
                first = mixed[2 * pair * block_len : (2 * pair + 1) * block_len]
                second = mixed[(2 * pair + 1) * block_len : (2 * pair + 2) * block_len]
                both = jnp.concatenate([first, second], axis=1)
                lower, upper = both[:packed], both[packed:]
                lane_range = slice(pair * 128, (pair + 1) * 128)
                kept[block, :, lane_range] = jnp.where(core == 0, lower, upper).astype(
                    jnp.bfloat16
                )
                given[block, :, lane_range] = jnp.where(core == 0, upper, lower).astype(
                    jnp.bfloat16
                )
            for head in range(heads):
                piece = slice(head * block_len, (head + 1) * block_len)
                logs[0, rows, head : head + 1] = span_log[piece]
                logs[1, rows, head : head + 1] = chosen_log[piece]

        in_width(
            counted - 1,
            [(width, width // packed) for width in (all_rows // 4, all_rows // 2, all_rows)],
            chosen_branch,
        )


def kernel_call(kernel, specs, operands, outputs, scratch, flops, room):
    return pl.pallas_call(
        kernel,
        out_shape=outputs,
        in_specs=[pl.BlockSpec(memory_space=space) for space in specs],
        out_specs=jax.tree.map(lambda _: pl.BlockSpec(memory_space=pltpu.VMEM), outputs),
        scratch_shapes=scratch,
        cost_estimate=pl.CostEstimate(flops=flops, bytes_accessed=4 << 20, transcendentals=0),
        compiler_params=pltpu.CompilerParams(vmem_limit_bytes=room << 20),
    )(*operands)


def turns(first_place, tok_rows, head_size):
    half_size = head_size // 2
    exact = rope_base ** (-np.arange(half_size) * 2.0 / head_size)
    within = np.arange(tok_rows)[:, None] * exact[None, :]
    start = first_place.astype(jnp.float32) * exact.astype(np.float32)
    return (
        jnp.cos(start)[None],
        jnp.sin(start)[None],
        jnp.asarray(np.stack([np.cos(within), np.sin(within)]).astype(np.float32)),
    )


def shards(
    tokens,
    query_weight,
    key_weight,
    value_weight,
    gate_weight,
    query_gain,
    key_gain,
    out_weight,
    shared_block,
    chosen_device,
):
    tok_rows = tokens.shape[0]
    head_size = query_gain.shape[0]
    width = query_weight.shape[1]
    head_count = width // head_size
    packed = SEL // 2
    local_blocks = tok_rows // SEL
    device = lax.axis_index(KV)
    far_count, near_count, y_count = (lax.axis_size(axis) for axis in KV)
    z_count = far_count * near_count
    sent_rows = SEL + tok_rows // CMP
    start_cosines, start_sines, within = turns(device * tok_rows, tok_rows, head_size)
    bf16, f32 = jnp.bfloat16, jnp.float32
    shape = jax.ShapeDtypeStruct
    vmem, smem = pltpu.VMEM, pltpu.SMEM

    sent, own = kernel_call(
        key_kernel,
        [smem] + [vmem] * 7,
        (shared_block, tokens, key_weight.T, value_weight.T, key_gain[None], start_cosines, start_sines, within),
        (shape((sent_rows, 128), bf16), shape((2, local_blocks, packed, 128), bf16)),
        (),
        10**9,
        KEY_ROOM,
    )
    far = lax.all_gather(sent, "z_far", axis=0, tiled=True)
    column = lax.all_gather(far, "z_near", axis=0, tiled=True)
    arrived = spread(column, "y").reshape(y_count, z_count, sent_rows, 128)

    tokens_later, own, start_cosines, start_sines, swap_weight, _ = lax.optimization_barrier(
        (tokens, own, start_cosines, start_sines, out_weight, column)
    )
    other_weight = lax.ppermute(swap_weight, "core", [(0, 1), (1, 0)])
    ready = kernel_call(
        query_kernel,
        [smem] + [vmem] * 7,
        (
            lax.axis_index(TP).reshape(1),
            tokens_later,
            query_weight,
            gate_weight.T,
            jnp.concatenate([query_gain, query_gain])[None],
            start_cosines,
            start_sines,
            within,
        ),
        shape((2 * (width // 128) + 1, tok_rows, 128), f32),
        (),
        10**9,
        QUERY_ROOM,
    )
    ready, other_weight = lax.optimization_barrier((ready, other_weight))
    kept, given, log_weight = kernel_call(
        functools.partial(attention_kernel, far_count),
        [smem, smem, vmem, vmem, vmem],
        (
            jnp.stack([device, lax.axis_index("core")]),
            chosen_device,
            arrived,
            ready,
            own,
        ),
        (
            shape((local_blocks, packed, width), bf16),
            shape((local_blocks, packed, width), bf16),
            shape((2, tok_rows, head_count), f32),
        ),
        (
            pltpu.VMEM((2, (chosen_device.shape[1] + 1) * packed, 128), bf16),
            pltpu.VMEM((y_count * z_count * (sent_rows - SEL), 128), bf16),
            pltpu.VMEM((head_count * SEL, head_size), f32),
            pltpu.VMEM((head_count * SEL, 1), f32),
        ),
        4 * 10**9,
        ATTENTION_ROOM,
    )
    taken = lax.ppermute(given, "core", [(0, 1), (1, 0)])
    own_partial = jnp.dot(
        kept.reshape(-1, width), out_weight, preferred_element_type=jnp.float32
    ).astype(bf16)
    other_partial = jnp.dot(
        taken.reshape(-1, width), other_weight, preferred_element_type=jnp.float32
    ).astype(bf16)
    pair_sum = (own_partial.astype(f32) + other_partial.astype(f32)).astype(bf16)
    pair_sum = pair_sum.reshape(local_blocks, packed, -1)
    pieces = lax.all_to_all(pair_sum, "x", split_axis=0, concat_axis=0, tiled=True)
    mixed_out = pieces.astype(f32).sum(axis=0).astype(bf16)
    return (mixed_out, log_weight)


def solution(mesh):
    torus = Mesh(mesh.devices.reshape(8, 4, 4, 4, 2), (*KV, *TP))
    return jax.shard_map(
        shards,
        mesh=torus,
        in_specs=(
            P(KV, None),
            P(None, TP),
            P(None, TP),
            P(None, TP),
            P(),
            P(),
            P(),
            P(TP, None),
            P(KV),
            P(KV, None),
        ),
        out_specs=(P((*KV, *TP), None), P(None, KV, TP)),
        check_vma=False,
    )
```

```python
import functools

import jax
import jax.numpy as jnp
import numpy as np
from jax import lax
from jax.experimental import pallas as pl
from jax.experimental.pallas import tpu as pltpu
from jax.sharding import Mesh
from jax.sharding import PartitionSpec as P

SEL = 64
CMP = 32
KV = ("z_far", "z_near", "y")
TP = ("x", "core")
KEY_ROOM = 60
QUERY_ROOM = 60
ATTENTION_ROOM = 12


norm_eps = 1e-06
rope_base = 500000.0
big_negative = -1e30


def spread(block, axis):
    count = lax.axis_size(axis)
    copies = lax.optimization_barrier(jnp.broadcast_to(block[None], (count, *block.shape)))
    return lax.all_to_all(copies, axis, split_axis=0, concat_axis=0, tiled=True)


def swapped(values_in):
    half_size = values_in.shape[-1] // 2
    return jnp.concatenate([values_in[:, half_size:], values_in[:, :half_size]], axis=1)


def repeated(halves, signs):
    return jnp.concatenate([sign * halves for sign in signs], axis=1)


def side_by_side(rows):
    half_size = rows.shape[0] // 2
    return jnp.concatenate([rows[:half_size], rows[half_size:]], axis=1)


def dot_last(left, right):
    return lax.dot_general(
        left, right, (((1,), (1,)), ((), ())), preferred_element_type=jnp.float32
    )


def turns_of(start_cosines, start_sines, within):
    cosines = start_cosines * within[0] - start_sines * within[1]
    sines = start_sines * within[0] + start_cosines * within[1]
    return cosines, sines


def key_kernel(pick, tokens, key_weight, value_weight, gain, start_cosines, start_sines, within, sent, own):
    _, blocks, packed, _ = own.shape
    tok_rows = tokens.shape[0]
    block_len = 2 * packed
    keys = dot_last(tokens[...], key_weight[...])
    keys = keys.astype(jnp.bfloat16).astype(jnp.float32)
    values = dot_last(tokens[...], value_weight[...]).astype(jnp.bfloat16)
    square = jnp.mean(keys * keys, axis=-1, keepdims=True)
    plain = (keys * lax.rsqrt(square + norm_eps) * gain[...]).astype(jnp.bfloat16)
    plain = plain.astype(jnp.float32)
    cosines, sines = turns_of(start_cosines[...], start_sines[...], within[...])
    turned = plain * repeated(cosines, (1, 1)) + swapped(plain) * repeated(sines, (-1, 1))
    turned = turned.astype(jnp.bfloat16)
    for block in range(blocks):
        rows = slice(block * block_len, (block + 1) * block_len)
        own[0, block] = side_by_side(turned[rows])
        own[1, block] = side_by_side(values[rows])
    both = jnp.concatenate([plain, values.astype(jnp.float32)], axis=1)
    spans = jnp.mean(both.reshape(tok_rows // CMP, CMP, both.shape[1]), axis=1)
    sent[:packed] = own[0, pick[0]]
    sent[packed:block_len] = own[1, pick[0]]
    sent[block_len:] = spans.astype(jnp.bfloat16)


def query_kernel(group, tokens, query_weight, gate_weight, gain, start_cosines, start_sines, within, ready):
    tok_rows = tokens.shape[0]
    width = query_weight.shape[1]
    gate_count = 2 * (width // 64)
    start = pl.multiple_of(group[0] * gate_count, gate_count)
    ready[2 * (width // 128), :, :gate_count] = jax.nn.sigmoid(
        dot_last(tokens[...], gate_weight[pl.ds(start, gate_count), :].astype(jnp.bfloat16))
    )
    lanes = lax.broadcasted_iota(jnp.int32, (tok_rows, 128), 1)
    cosines, sines = turns_of(start_cosines[...], start_sines[...], within[...])
    cos_lanes = repeated(cosines, (1, 1, 1, 1))
    sin_lanes = repeated(sines, (-1, 1, -1, 1))
    for pair in range(width // 128):
        queries = jnp.dot(
            tokens[...],
            query_weight[:, pair * 128 : (pair + 1) * 128],
            preferred_element_type=jnp.float32,
        )
        queries = queries.astype(jnp.bfloat16).astype(jnp.float32)
        squares = queries * queries
        first = jnp.sum(jnp.where(lanes < 64, squares, 0.0), axis=-1, keepdims=True)
        second = jnp.sum(jnp.where(lanes < 64, 0.0, squares), axis=-1, keepdims=True)
        square = jnp.where(lanes < 64, first, second) * (1.0 / 64)
        plain = (queries * lax.rsqrt(square + norm_eps) * gain[...]).astype(jnp.bfloat16)
        plain = plain.astype(jnp.float32)
        ready[pair] = plain
        partner = jnp.where(
            lanes % 64 < 32, pltpu.roll(plain, 96, axis=1), pltpu.roll(plain, 32, axis=1)
        )
        turned = plain * cos_lanes + partner * sin_lanes
        ready[width // 128 + pair] = turned.astype(jnp.bfloat16).astype(jnp.float32)


def one_sided(queries, upper):
    pieces = []
    lanes = lax.broadcasted_iota(jnp.int32, queries[0].shape, 1)
    keep = (lanes >= 64) if upper else (lanes < 64)
    for both in queries:
        turned = swapped(both)
        for piece in (turned, both) if upper else (both, turned):
            pieces.append(jnp.where(keep, piece, 0.0).astype(jnp.bfloat16))
    return jnp.concatenate(pieces, axis=0)


def attention_kernel(
    far_count,
    place_of,
    chosen,
    arrived,
    ready,
    own,
    kept,
    given,
    logs,
    chosen_rows,
    spans,
    span_part,
):
    device, core = place_of[0], place_of[1]
    blocks, named = chosen.shape
    _, _, packed, _ = own.shape
    y_count, z_count, sent_rows, _ = arrived.shape
    block_len = 2 * packed
    pairs = kept.shape[2] // 128
    heads = 2 * pairs
    tok_rows = blocks * block_len
    span_rows = sent_rows - block_len
    near_count = z_count // far_count
    score_scale = 64 ** (-0.5)
    all_spans = spans.shape[0]
    all_rows = chosen_rows.shape[2]

    near_bits, y_bits = near_count.bit_length() - 1, y_count.bit_length() - 1

    def slot_of(z):
        return (z & (near_count - 1)) * far_count + (z >> near_bits)

    plane_rows = y_count * span_rows
    for first in range(0, z_count, far_count):

        @pl.when(first << y_bits <= device)
        def _():
            for z in range(first, first + far_count):
                plane = jnp.concatenate(
                    [
                        arrived[y, slot_of(z), block_len:, :].astype(jnp.float32)
                        for y in range(y_count)
                    ],
                    axis=0,
                )
                spans[z * plane_rows : (z + 1) * plane_rows] = plane.astype(jnp.bfloat16)

        @pl.when(first << y_bits > device)
        def _():
            rows = slice(first * plane_rows, (first + far_count) * plane_rows)
            spans[rows] = jnp.zeros((far_count * plane_rows, 128), jnp.bfloat16)

    chosen_rows[...] = jnp.zeros_like(chosen_rows)

    def gate_columns(rows, branch):
        gate_rows = ready[2 * pairs, rows, :]
        return jnp.concatenate(
            [gate_rows[:, 2 * head + branch : 2 * head + branch + 1] for head in range(heads)],
            axis=0,
        )

    def span_branch(first_row, length, width):
        rows = pl.ds(first_row, length)
        scores = dot_last(
            one_sided([ready[pair, rows, :] for pair in range(pairs)], False), spans[:width]
        )
        row_place = lax.broadcasted_iota(jnp.int32, (heads * length, 1), 0) % length
        places = device * tok_rows + first_row + row_place
        has_span = places >= CMP - 1
        span_ends = lax.broadcasted_iota(jnp.int32, (1, width), 1) * CMP + CMP - 1
        scores = jnp.where(span_ends <= places, scores * score_scale, big_negative)
        peak = jnp.max(scores, axis=-1, keepdims=True)
        raw = jnp.exp(scores - peak)
        total = jnp.where(has_span, jnp.sum(raw, axis=-1, keepdims=True), 1.0)
        summed = jnp.dot(
            raw.astype(jnp.bfloat16), spans[:width], preferred_element_type=jnp.float32
        )
        summed = jnp.where(has_span, gate_columns(rows, 0) * (summed[:, 64:] / total), 0.0)
        span_log = jnp.where(has_span, peak + jnp.log(total), 0.0)
        for head in range(heads):
            piece = slice(head * length, (head + 1) * length)
            span_part[head, rows, :] = summed[piece]
            logs[0, rows, head : head + 1] = span_log[piece]

    few_spans = all_spans // 4
    few = (device + 1) * span_rows <= few_spans

    @pl.when(few)
    def _():
        for part in range(2):
            span_branch(part * (tok_rows // 2), tok_rows // 2, few_spans)

    @pl.when(jnp.logical_not(few))
    def _():
        @pl.loop(0, blocks)
        def _(block):
            span_branch(pl.multiple_of(block * block_len, block_len), block_len, all_spans)

    row_place = lax.broadcasted_iota(jnp.int32, (heads * block_len, 1), 0) % block_len
    lanes = lax.broadcasted_iota(jnp.int32, (heads * block_len, all_rows), 1)

    def chosen_branch(block, keys, values):
        rows = pl.ds(pl.multiple_of(block * block_len, block_len), block_len)
        keys[:packed] = own[0, block]
        values[:packed] = own[1, block]
        counted = jnp.int32(1)
        for number in range(named):
            source = chosen[block, number]
            start = pl.multiple_of(counted * packed, packed)
            y, slot = source & (y_count - 1), slot_of(source >> y_bits)
            keys[pl.ds(start, packed)] = arrived[y, slot, :packed, :]
            values[pl.ds(start, packed)] = arrived[y, slot, packed:block_len, :]
            counted = counted + jnp.where(source < device, 1, 0)
        queries = [ready[pairs + pair, rows, :] for pair in range(pairs)]
        half_scores = []
        blocked = jnp.where(lanes[:1] < counted * packed, 0.0, big_negative)
        for upper in (False, True):
            scores = dot_last(one_sided(queries, upper), keys[...])
            scores = scores * score_scale + blocked
            later = (lanes < packed) & (lanes + packed * upper > row_place)
            half_scores.append(jnp.where(later, big_negative, scores))
        peak = jnp.maximum(
            jnp.max(half_scores[0], axis=-1, keepdims=True),
            jnp.max(half_scores[1], axis=-1, keepdims=True),
        )
        total = 0.0
        products = []
        for upper in range(2):
            raw = jnp.exp(half_scores[upper] - peak)
            total = total + jnp.sum(raw, axis=-1, keepdims=True)
            products.append(
                jnp.dot(raw.astype(jnp.bfloat16), values[...], preferred_element_type=jnp.float32)
            )
        summed = products[0][:, :64] + products[1][:, 64:]
        scaled = gate_columns(rows, 1) * (summed / total)
        chosen_log = peak + jnp.log(total)
        pieces = []
        for head in range(heads):
            piece = slice(head * block_len, (head + 1) * block_len)
            logs[1, rows, head : head + 1] = chosen_log[piece]
            pieces.append(span_part[head, rows, :] + scaled[piece])
        for pair in range(pairs):
            both = jnp.concatenate([pieces[2 * pair], pieces[2 * pair + 1]], axis=1)
            lower, upper = both[:packed], both[packed:]
            lane_range = slice(pair * 128, (pair + 1) * 128)
            kept[block, :, lane_range] = jnp.where(core == 0, lower, upper).astype(jnp.bfloat16)
            given[block, :, lane_range] = jnp.where(core == 0, upper, lower).astype(jnp.bfloat16)

    side = chosen_rows.shape[0]

    @pl.loop(0, blocks // side)
    def _(step):
        for number in range(side):
            chosen_branch(
                step * side + number, chosen_rows.at[number, 0], chosen_rows.at[number, 1]
            )


def kernel_call(kernel, specs, operands, outputs, scratch, flops, room):
    return pl.pallas_call(
        kernel,
        out_shape=outputs,
        in_specs=[pl.BlockSpec(memory_space=space) for space in specs],
        out_specs=jax.tree.map(lambda _: pl.BlockSpec(memory_space=pltpu.VMEM), outputs),
        scratch_shapes=scratch,
        cost_estimate=pl.CostEstimate(flops=flops, bytes_accessed=4 << 20, transcendentals=0),
        compiler_params=pltpu.CompilerParams(vmem_limit_bytes=room << 20),
    )(*operands)


def turns(first_place, tok_rows, head_size):
    half_size = head_size // 2
    exact = rope_base ** (-np.arange(half_size) * 2.0 / head_size)
    within = np.arange(tok_rows)[:, None] * exact[None, :]
    start = first_place.astype(jnp.float32) * exact.astype(np.float32)
    return (
        jnp.cos(start)[None],
        jnp.sin(start)[None],
        jnp.asarray(np.stack([np.cos(within), np.sin(within)]).astype(np.float32)),
    )


def shards(
    tokens,
    query_weight,
    key_weight,
    value_weight,
    gate_weight,
    query_gain,
    key_gain,
    out_weight,
    shared_block,
    chosen_device,
):
    tok_rows = tokens.shape[0]
    head_size = query_gain.shape[0]
    width = query_weight.shape[1]
    head_count = width // head_size
    packed = SEL // 2
    local_blocks = tok_rows // SEL
    device = lax.axis_index(KV)
    far_count, near_count, y_count = (lax.axis_size(axis) for axis in KV)
    z_count = far_count * near_count
    sent_rows = SEL + tok_rows // CMP
    start_cosines, start_sines, within = turns(device * tok_rows, tok_rows, head_size)
    bf16, f32 = jnp.bfloat16, jnp.float32
    shape = jax.ShapeDtypeStruct
    vmem, smem = pltpu.VMEM, pltpu.SMEM

    sent, own = kernel_call(
        key_kernel,
        [smem] + [vmem] * 7,
        (shared_block, tokens, key_weight.T, value_weight.T, key_gain[None], start_cosines, start_sines, within),
        (shape((sent_rows, 128), bf16), shape((2, local_blocks, packed, 128), bf16)),
        (),
        10**9,
        KEY_ROOM,
    )
    far = lax.all_gather(sent, "z_far", axis=0, tiled=True)
    column = lax.all_gather(far, "z_near", axis=0, tiled=True)
    arrived = spread(column, "y").reshape(y_count, z_count, sent_rows, 128)

    tokens_later, own, start_cosines, start_sines, swap_weight, _ = lax.optimization_barrier(
        (tokens, own, start_cosines, start_sines, out_weight, column)
    )
    other_weight = lax.ppermute(swap_weight, "core", [(0, 1), (1, 0)])
    ready = kernel_call(
        query_kernel,
        [smem] + [vmem] * 7,
        (
            lax.axis_index(TP).reshape(1),
            tokens_later,
            query_weight,
            gate_weight.T,
            jnp.concatenate([query_gain, query_gain])[None],
            start_cosines,
            start_sines,
            within,
        ),
        shape((2 * (width // 128) + 1, tok_rows, 128), f32),
        (),
        10**9,
        QUERY_ROOM,
    )
    ready, other_weight = lax.optimization_barrier((ready, other_weight))
    kept, given, log_weight = kernel_call(
        functools.partial(attention_kernel, far_count),
        [smem, smem, vmem, vmem, vmem],
        (
            jnp.stack([device, lax.axis_index("core")]),
            chosen_device,
            arrived,
            ready,
            own,
        ),
        (
            shape((local_blocks, packed, width), bf16),
            shape((local_blocks, packed, width), bf16),
            shape((2, tok_rows, head_count), f32),
        ),
        (
            pltpu.VMEM((2, 2, (chosen_device.shape[1] + 1) * packed, 128), bf16),
            pltpu.VMEM((y_count * z_count * (sent_rows - SEL), 128), bf16),
            pltpu.VMEM((head_count, tok_rows, head_size), f32),
        ),
        4 * 10**9,
        ATTENTION_ROOM,
    )
    taken = lax.ppermute(given, "core", [(0, 1), (1, 0)])
    own_partial = jnp.dot(
        kept.reshape(-1, width), out_weight, preferred_element_type=jnp.float32
    ).astype(bf16)
    other_partial = jnp.dot(
        taken.reshape(-1, width), other_weight, preferred_element_type=jnp.float32
    ).astype(bf16)
    pair_sum = (own_partial.astype(f32) + other_partial.astype(f32)).astype(bf16)
    pair_sum = pair_sum.reshape(local_blocks, packed, -1)
    pieces = lax.all_to_all(pair_sum, "x", split_axis=0, concat_axis=0, tiled=True)
    mixed_out = pieces.astype(f32).sum(axis=0).astype(bf16)
    return (mixed_out, log_weight)


def solution(mesh):
    torus = Mesh(mesh.devices.reshape(8, 4, 4, 4, 2), (*KV, *TP))
    return jax.shard_map(
        shards,
        mesh=torus,
        in_specs=(
            P(KV, None),
            P(None, TP),
            P(None, TP),
            P(None, TP),
            P(),
            P(),
            P(),
            P(TP, None),
            P(KV),
            P(KV, None),
        ),
        out_specs=(P((*KV, *TP), None), P(None, KV, TP)),
        check_vma=False,
    )
```

```python
import functools

import jax
import jax.numpy as jnp
import numpy as np
from jax import lax
from jax.experimental import pallas as pl
from jax.experimental.pallas import tpu as pltpu
from jax.sharding import Mesh
from jax.sharding import PartitionSpec as P

SEL = 64
CMP = 32
KV = ("z_far", "z_near", "y")
TP = ("x", "core")
KEY_ROOM = 60
QUERY_ROOM = 60
ATTENTION_ROOM = 12


norm_eps = 1e-06
rope_base = 500000.0
big_negative = -1e30


def spread(block, axis):
    count = lax.axis_size(axis)
    copies = lax.optimization_barrier(jnp.broadcast_to(block[None], (count, *block.shape)))
    return lax.all_to_all(copies, axis, split_axis=0, concat_axis=0, tiled=True)


def swapped(values_in):
    half_size = values_in.shape[-1] // 2
    return jnp.concatenate([values_in[:, half_size:], values_in[:, :half_size]], axis=1)


def repeated(halves, signs):
    return jnp.concatenate([sign * halves for sign in signs], axis=1)


def side_by_side(rows):
    half_size = rows.shape[0] // 2
    return jnp.concatenate([rows[:half_size], rows[half_size:]], axis=1)


def dot_last(left, right):
    return lax.dot_general(
        left, right, (((1,), (1,)), ((), ())), preferred_element_type=jnp.float32
    )


def turns_of(device, starts, within):
    start_cosines = starts[0, pl.ds(device, 1), :]
    start_sines = starts[1, pl.ds(device, 1), :]
    cosines = start_cosines * within[0] - start_sines * within[1]
    sines = start_sines * within[0] + start_cosines * within[1]
    return cosines, sines


def key_kernel(device, pick, tokens, key_weight, value_weight, gain, starts, within, sent, own):
    _, blocks, packed, _ = own.shape
    tok_rows = tokens.shape[0]
    block_len = 2 * packed
    keys = dot_last(tokens[...], key_weight[...])
    keys = keys.astype(jnp.bfloat16).astype(jnp.float32)
    values = dot_last(tokens[...], value_weight[...]).astype(jnp.bfloat16)
    square = jnp.mean(keys * keys, axis=-1, keepdims=True)
    plain = (keys * lax.rsqrt(square + norm_eps) * gain[...]).astype(jnp.bfloat16)
    plain = plain.astype(jnp.float32)
    cosines, sines = turns_of(device[0], starts, within)
    turned = plain * repeated(cosines, (1, 1)) + swapped(plain) * repeated(sines, (-1, 1))
    turned = turned.astype(jnp.bfloat16)
    for block in range(blocks):
        rows = slice(block * block_len, (block + 1) * block_len)
        own[0, block] = side_by_side(turned[rows])
        own[1, block] = side_by_side(values[rows])
    both = jnp.concatenate([plain, values.astype(jnp.float32)], axis=1)
    spans = jnp.mean(both.reshape(tok_rows // CMP, CMP, both.shape[1]), axis=1)
    sent[:packed] = own[0, pick[0]]
    sent[packed:block_len] = own[1, pick[0]]
    sent[block_len:] = spans.astype(jnp.bfloat16)


def query_kernel(device, group, tokens, query_weight, gate_weight, gain, starts, within, ready):
    tok_rows = tokens.shape[0]
    width = query_weight.shape[1]
    gate_count = 2 * (width // 64)
    start = pl.multiple_of(group[0] * gate_count, gate_count)
    ready[2 * (width // 128), :, :gate_count] = jax.nn.sigmoid(
        dot_last(tokens[...], gate_weight[pl.ds(start, gate_count), :].astype(jnp.bfloat16))
    )
    lanes = lax.broadcasted_iota(jnp.int32, (tok_rows, 128), 1)
    cosines, sines = turns_of(device[0], starts, within)
    cos_lanes = repeated(cosines, (1, 1, 1, 1))
    sin_lanes = repeated(sines, (-1, 1, -1, 1))
    for pair in range(width // 128):
        queries = jnp.dot(
            tokens[...],
            query_weight[:, pair * 128 : (pair + 1) * 128],
            preferred_element_type=jnp.float32,
        )
        queries = queries.astype(jnp.bfloat16).astype(jnp.float32)
        squares = queries * queries
        first = jnp.sum(jnp.where(lanes < 64, squares, 0.0), axis=-1, keepdims=True)
        second = jnp.sum(jnp.where(lanes < 64, 0.0, squares), axis=-1, keepdims=True)
        square = jnp.where(lanes < 64, first, second) * (1.0 / 64)
        plain = (queries * lax.rsqrt(square + norm_eps) * gain[...]).astype(jnp.bfloat16)
        plain = plain.astype(jnp.float32)
        ready[pair] = plain
        partner = jnp.where(
            lanes % 64 < 32, pltpu.roll(plain, 96, axis=1), pltpu.roll(plain, 32, axis=1)
        )
        turned = plain * cos_lanes + partner * sin_lanes
        ready[width // 128 + pair] = turned.astype(jnp.bfloat16).astype(jnp.float32)


def one_sided(queries, upper):
    pieces = []
    lanes = lax.broadcasted_iota(jnp.int32, queries[0].shape, 1)
    keep = (lanes >= 64) if upper else (lanes < 64)
    for both in queries:
        turned = swapped(both)
        for piece in (turned, both) if upper else (both, turned):
            pieces.append(jnp.where(keep, piece, 0.0).astype(jnp.bfloat16))
    return jnp.concatenate(pieces, axis=0)


def attention_kernel(
    far_count,
    place_of,
    chosen,
    arrived,
    ready,
    own,
    kept,
    given,
    logs,
    chosen_rows,
    spans,
    span_part,
):
    device, core = place_of[0], place_of[1]
    blocks, named = chosen.shape
    _, _, packed, _ = own.shape
    y_count, z_count, sent_rows, _ = arrived.shape
    block_len = 2 * packed
    pairs = kept.shape[2] // 128
    heads = 2 * pairs
    tok_rows = blocks * block_len
    span_rows = sent_rows - block_len
    near_count = z_count // far_count
    score_scale = 64 ** (-0.5)
    all_spans = spans.shape[0]
    all_rows = chosen_rows.shape[2]

    near_bits, y_bits = near_count.bit_length() - 1, y_count.bit_length() - 1

    def slot_of(z):
        return (z & (near_count - 1)) * far_count + (z >> near_bits)

    plane_rows = y_count * span_rows
    for first in range(0, z_count, far_count):

        @pl.when(first << y_bits <= device)
        def _():
            for z in range(first, first + far_count):
                plane = jnp.concatenate(
                    [
                        arrived[y, slot_of(z), block_len:, :].astype(jnp.float32)
                        for y in range(y_count)
                    ],
                    axis=0,
                )
                spans[z * plane_rows : (z + 1) * plane_rows] = plane.astype(jnp.bfloat16)

        @pl.when(first << y_bits > device)
        def _():
            rows = slice(first * plane_rows, (first + far_count) * plane_rows)
            spans[rows] = jnp.zeros((far_count * plane_rows, 128), jnp.bfloat16)

    chosen_rows[...] = jnp.zeros_like(chosen_rows)

    def gate_columns(rows, branch):
        gate_rows = ready[2 * pairs, rows, :]
        return jnp.concatenate(
            [gate_rows[:, 2 * head + branch : 2 * head + branch + 1] for head in range(heads)],
            axis=0,
        )

    def span_branch(first_row, length, width):
        rows = pl.ds(first_row, length)
        scores = dot_last(
            one_sided([ready[pair, rows, :] for pair in range(pairs)], False), spans[:width]
        )
        row_place = lax.broadcasted_iota(jnp.int32, (heads * length, 1), 0) % length
        places = device * tok_rows + first_row + row_place
        has_span = places >= CMP - 1
        span_ends = lax.broadcasted_iota(jnp.int32, (1, width), 1) * CMP + CMP - 1
        scores = jnp.where(span_ends <= places, scores * score_scale, big_negative)
        peak = jnp.max(scores, axis=-1, keepdims=True)
        raw = jnp.exp(scores - peak)
        total = jnp.where(has_span, jnp.sum(raw, axis=-1, keepdims=True), 1.0)
        summed = jnp.dot(
            raw.astype(jnp.bfloat16), spans[:width], preferred_element_type=jnp.float32
        )
        summed = jnp.where(has_span, gate_columns(rows, 0) * (summed[:, 64:] / total), 0.0)
        span_log = jnp.where(has_span, peak + jnp.log(total), 0.0)
        for head in range(heads):
            piece = slice(head * length, (head + 1) * length)
            span_part[head, rows, :] = summed[piece]
            logs[0, rows, head : head + 1] = span_log[piece]

    few_spans = all_spans // 4
    few = (device + 1) * span_rows <= few_spans

    @pl.when(few)
    def _():
        for part in range(2):
            span_branch(part * (tok_rows // 2), tok_rows // 2, few_spans)

    @pl.when(jnp.logical_not(few))
    def _():
        @pl.loop(0, blocks)
        def _(block):
            span_branch(pl.multiple_of(block * block_len, block_len), block_len, all_spans)

    row_place = lax.broadcasted_iota(jnp.int32, (heads * block_len, 1), 0) % block_len
    lanes = lax.broadcasted_iota(jnp.int32, (heads * block_len, all_rows), 1)

    def chosen_branch(block, keys, values):
        rows = pl.ds(pl.multiple_of(block * block_len, block_len), block_len)
        keys[:packed] = own[0, block]
        values[:packed] = own[1, block]
        counted = jnp.int32(1)
        for number in range(named):
            source = chosen[block, number]
            start = pl.multiple_of(counted * packed, packed)
            y, slot = source & (y_count - 1), slot_of(source >> y_bits)
            keys[pl.ds(start, packed)] = arrived[y, slot, :packed, :]
            values[pl.ds(start, packed)] = arrived[y, slot, packed:block_len, :]
            counted = counted + jnp.where(source < device, 1, 0)
        queries = [ready[pairs + pair, rows, :] for pair in range(pairs)]
        half_scores = []
        blocked = jnp.where(lanes[:1] < counted * packed, 0.0, big_negative)
        for upper in (False, True):
            scores = dot_last(one_sided(queries, upper), keys[...])
            scores = scores * score_scale + blocked
            later = (lanes < packed) & (lanes + packed * upper > row_place)
            half_scores.append(jnp.where(later, big_negative, scores))
        peak = jnp.maximum(
            jnp.max(half_scores[0], axis=-1, keepdims=True),
            jnp.max(half_scores[1], axis=-1, keepdims=True),
        )
        total = 0.0
        products = []
        for upper in range(2):
            raw = jnp.exp(half_scores[upper] - peak)
            total = total + jnp.sum(raw, axis=-1, keepdims=True)
            products.append(
                jnp.dot(raw.astype(jnp.bfloat16), values[...], preferred_element_type=jnp.float32)
            )
        summed = products[0][:, :64] + products[1][:, 64:]
        scaled = gate_columns(rows, 1) * (summed / total)
        chosen_log = peak + jnp.log(total)
        pieces = []
        for head in range(heads):
            piece = slice(head * block_len, (head + 1) * block_len)
            logs[1, rows, head : head + 1] = chosen_log[piece]
            pieces.append(span_part[head, rows, :] + scaled[piece])
        for pair in range(pairs):
            both = jnp.concatenate([pieces[2 * pair], pieces[2 * pair + 1]], axis=1)
            lower, upper = both[:packed], both[packed:]
            lane_range = slice(pair * 128, (pair + 1) * 128)
            kept[block, :, lane_range] = jnp.where(core == 0, lower, upper).astype(jnp.bfloat16)
            given[block, :, lane_range] = jnp.where(core == 0, upper, lower).astype(jnp.bfloat16)

    side = chosen_rows.shape[0]

    @pl.loop(0, blocks // side)
    def _(step):
        for number in range(side):
            chosen_branch(
                step * side + number, chosen_rows.at[number, 0], chosen_rows.at[number, 1]
            )


def kernel_call(kernel, specs, operands, outputs, scratch, flops, room):
    return pl.pallas_call(
        kernel,
        out_shape=outputs,
        in_specs=[pl.BlockSpec(memory_space=space) for space in specs],
        out_specs=jax.tree.map(lambda _: pl.BlockSpec(memory_space=pltpu.VMEM), outputs),
        scratch_shapes=scratch,
        cost_estimate=pl.CostEstimate(flops=flops, bytes_accessed=4 << 20, transcendentals=0),
        compiler_params=pltpu.CompilerParams(vmem_limit_bytes=room << 20),
    )(*operands)


def turns(devices, tok_rows, head_size):
    half_size = head_size // 2
    inverse = rope_base ** (-np.arange(half_size) * 2.0 / head_size)

    def table(places):
        angles = places[:, None] * inverse[None, :]
        return jnp.asarray(np.stack([np.cos(angles), np.sin(angles)]).astype(np.float32))

    return table(np.arange(devices) * tok_rows), table(np.arange(tok_rows))


def shards(
    tokens,
    query_weight,
    key_weight,
    value_weight,
    gate_weight,
    query_gain,
    key_gain,
    out_weight,
    shared_block,
    chosen_device,
):
    tok_rows = tokens.shape[0]
    head_size = query_gain.shape[0]
    width = query_weight.shape[1]
    head_count = width // head_size
    packed = SEL // 2
    local_blocks = tok_rows // SEL
    device = lax.axis_index(KV)
    far_count, near_count, y_count = (lax.axis_size(axis) for axis in KV)
    z_count = far_count * near_count
    sent_rows = SEL + tok_rows // CMP
    starts, within = turns(z_count * y_count, tok_rows, head_size)
    bf16, f32 = jnp.bfloat16, jnp.float32
    shape = jax.ShapeDtypeStruct
    vmem, smem = pltpu.VMEM, pltpu.SMEM

    sent, own = kernel_call(
        key_kernel,
        [smem] * 2 + [vmem] * 6,
        (
            device.reshape(1),
            shared_block,
            tokens,
            key_weight.T,
            value_weight.T,
            key_gain[None],
            starts,
            within,
        ),
        (shape((sent_rows, 128), bf16), shape((2, local_blocks, packed, 128), bf16)),
        (),
        10**9,
        KEY_ROOM,
    )
    far = lax.all_gather(sent, "z_far", axis=0, tiled=True)
    column = lax.all_gather(far, "z_near", axis=0, tiled=True)
    arrived = spread(column, "y").reshape(y_count, z_count, sent_rows, 128)

    tokens_later, own, swap_weight, _ = lax.optimization_barrier(
        (tokens, own, out_weight, column)
    )
    other_weight = lax.ppermute(swap_weight, "core", [(0, 1), (1, 0)])
    ready = kernel_call(
        query_kernel,
        [smem] * 2 + [vmem] * 6,
        (
            device.reshape(1),
            lax.axis_index(TP).reshape(1),
            tokens_later,
            query_weight,
            gate_weight.T,
            jnp.concatenate([query_gain, query_gain])[None],
            starts,
            within,
        ),
        shape((2 * (width // 128) + 1, tok_rows, 128), f32),
        (),
        10**9,
        QUERY_ROOM,
    )
    ready, other_weight = lax.optimization_barrier((ready, other_weight))
    kept, given, log_weight = kernel_call(
        functools.partial(attention_kernel, far_count),
        [smem, smem, vmem, vmem, vmem],
        (
            jnp.stack([device, lax.axis_index("core")]),
            chosen_device,
            arrived,
            ready,
            own,
        ),
        (
            shape((local_blocks, packed, width), bf16),
            shape((local_blocks, packed, width), bf16),
            shape((2, tok_rows, head_count), f32),
        ),
        (
            pltpu.VMEM((2, 2, (chosen_device.shape[1] + 1) * packed, 128), bf16),
            pltpu.VMEM((y_count * z_count * (sent_rows - SEL), 128), bf16),
            pltpu.VMEM((head_count, tok_rows, head_size), f32),
        ),
        4 * 10**9,
        ATTENTION_ROOM,
    )
    taken = lax.ppermute(given, "core", [(0, 1), (1, 0)])
    own_partial = jnp.dot(
        kept.reshape(-1, width), out_weight, preferred_element_type=jnp.float32
    ).astype(bf16)
    other_partial = jnp.dot(
        taken.reshape(-1, width), other_weight, preferred_element_type=jnp.float32
    ).astype(bf16)
    pair_sum = (own_partial.astype(f32) + other_partial.astype(f32)).astype(bf16)
    pair_sum = pair_sum.reshape(local_blocks, packed, -1)
    pieces = lax.all_to_all(pair_sum, "x", split_axis=0, concat_axis=0, tiled=True)
    mixed_out = pieces.astype(f32).sum(axis=0).astype(bf16)
    return (mixed_out, log_weight)


def solution(mesh):
    torus = Mesh(mesh.devices.reshape(8, 4, 4, 4, 2), (*KV, *TP))
    return jax.shard_map(
        shards,
        mesh=torus,
        in_specs=(
            P(KV, None),
            P(None, TP),
            P(None, TP),
            P(None, TP),
            P(),
            P(),
            P(),
            P(TP, None),
            P(KV),
            P(KV, None),
        ),
        out_specs=(P((*KV, *TP), None), P(None, KV, TP)),
        check_vma=False,
    )
```

```python
import functools

import jax
import jax.numpy as jnp
import numpy as np
from jax import lax
from jax.experimental import pallas as pl
from jax.experimental.pallas import tpu as pltpu
from jax.sharding import Mesh
from jax.sharding import PartitionSpec as P

SEL = 64
CMP = 32
KV = ("z_far", "z_near", "y")
TP = ("x", "core")
KEY_ROOM = 60
QUERY_ROOM = 60
ATTENTION_ROOM = 12


norm_eps = 1e-06
rope_base = 500000.0
big_negative = -1e30


def spread(block, axis):
    count = lax.axis_size(axis)
    copies = lax.optimization_barrier(jnp.broadcast_to(block[None], (count, *block.shape)))
    return lax.all_to_all(copies, axis, split_axis=0, concat_axis=0, tiled=True)


def swapped(values_in):
    half_size = values_in.shape[-1] // 2
    return jnp.concatenate([values_in[:, half_size:], values_in[:, :half_size]], axis=1)


def repeated(halves, signs):
    return jnp.concatenate([sign * halves for sign in signs], axis=1)


def side_by_side(rows):
    half_size = rows.shape[0] // 2
    return jnp.concatenate([rows[:half_size], rows[half_size:]], axis=1)


def dot_last(left, right):
    return lax.dot_general(
        left, right, (((1,), (1,)), ((), ())), preferred_element_type=jnp.float32
    )


def turns_of(device, starts, within):
    start_cosines = starts[0, pl.ds(device, 1), :]
    start_sines = starts[1, pl.ds(device, 1), :]
    cosines = start_cosines * within[0] - start_sines * within[1]
    sines = start_sines * within[0] + start_cosines * within[1]
    return cosines, sines


def key_kernel(device, pick, tokens, key_weight, value_weight, gain, starts, within, sent, own):
    _, blocks, packed, _ = own.shape
    tok_rows = tokens.shape[0]
    block_len = 2 * packed
    keys = dot_last(tokens[...], key_weight[...])
    keys = keys.astype(jnp.bfloat16).astype(jnp.float32)
    values = dot_last(tokens[...], value_weight[...]).astype(jnp.bfloat16)
    square = jnp.mean(keys * keys, axis=-1, keepdims=True)
    plain = (keys * lax.rsqrt(square + norm_eps) * gain[...]).astype(jnp.bfloat16)
    plain = plain.astype(jnp.float32)
    cosines, sines = turns_of(device[0], starts, within)
    turned = plain * repeated(cosines, (1, 1)) + swapped(plain) * repeated(sines, (-1, 1))
    turned = turned.astype(jnp.bfloat16)
    for block in range(blocks):
        rows = slice(block * block_len, (block + 1) * block_len)
        own[0, block] = side_by_side(turned[rows])
        own[1, block] = side_by_side(values[rows])
    both = jnp.concatenate([plain, values.astype(jnp.float32)], axis=1)
    spans = jnp.mean(both.reshape(tok_rows // CMP, CMP, both.shape[1]), axis=1)
    sent[:packed] = own[0, pick[0]]
    sent[packed:block_len] = own[1, pick[0]]
    sent[block_len:] = spans.astype(jnp.bfloat16)


def query_kernel(device, group, tokens, query_weight, gate_weight, gain, starts, within, ready):
    tok_rows = tokens.shape[0]
    width = query_weight.shape[1]
    gate_count = 2 * (width // 64)
    start = pl.multiple_of(group[0] * gate_count, gate_count)
    ready[2 * (width // 128), :, :gate_count] = jax.nn.sigmoid(
        dot_last(tokens[...], gate_weight[pl.ds(start, gate_count), :].astype(jnp.bfloat16))
    )
    lanes = lax.broadcasted_iota(jnp.int32, (tok_rows, 128), 1)
    cosines, sines = turns_of(device[0], starts, within)
    cos_lanes = repeated(cosines, (1, 1, 1, 1))
    sin_lanes = repeated(sines, (-1, 1, -1, 1))
    for pair in range(width // 128):
        queries = jnp.dot(
            tokens[...],
            query_weight[:, pair * 128 : (pair + 1) * 128],
            preferred_element_type=jnp.float32,
        )
        queries = queries.astype(jnp.bfloat16).astype(jnp.float32)
        squares = queries * queries
        first = jnp.sum(jnp.where(lanes < 64, squares, 0.0), axis=-1, keepdims=True)
        second = jnp.sum(jnp.where(lanes < 64, 0.0, squares), axis=-1, keepdims=True)
        square = jnp.where(lanes < 64, first, second) * (1.0 / 64)
        plain = (queries * lax.rsqrt(square + norm_eps) * gain[...]).astype(jnp.bfloat16)
        plain = plain.astype(jnp.float32)
        ready[pair] = plain
        partner = jnp.where(
            lanes % 64 < 32, pltpu.roll(plain, 96, axis=1), pltpu.roll(plain, 32, axis=1)
        )
        turned = plain * cos_lanes + partner * sin_lanes
        ready[width // 128 + pair] = turned.astype(jnp.bfloat16).astype(jnp.float32)


def one_sided(queries, upper):
    pieces = []
    lanes = lax.broadcasted_iota(jnp.int32, queries[0].shape, 1)
    keep = (lanes >= 64) if upper else (lanes < 64)
    for both in queries:
        turned = swapped(both)
        for piece in (turned, both) if upper else (both, turned):
            pieces.append(jnp.where(keep, piece, 0.0).astype(jnp.bfloat16))
    return jnp.concatenate(pieces, axis=0)


def attention_kernel(
    far_count,
    place_of,
    chosen,
    arrived,
    ready,
    own,
    kept,
    given,
    logs,
    chosen_rows,
    spans,
    span_part,
):
    device, core = place_of[0], place_of[1]
    blocks, named = chosen.shape
    _, _, packed, _ = own.shape
    y_count, z_count, sent_rows, _ = arrived.shape
    block_len = 2 * packed
    pairs = kept.shape[2] // 128
    heads = 2 * pairs
    tok_rows = blocks * block_len
    span_rows = sent_rows - block_len
    near_count = z_count // far_count
    score_scale = 64 ** (-0.5)
    all_spans = spans.shape[0]
    all_rows = chosen_rows.shape[2]

    near_bits, y_bits = near_count.bit_length() - 1, y_count.bit_length() - 1

    def slot_of(z):
        return (z & (near_count - 1)) * far_count + (z >> near_bits)

    plane_rows = y_count * span_rows
    for first in range(0, z_count, far_count):

        @pl.when(first << y_bits <= device)
        def _():
            for z in range(first, first + far_count):
                plane = jnp.concatenate(
                    [
                        arrived[y, slot_of(z), block_len:, :].astype(jnp.float32)
                        for y in range(y_count)
                    ],
                    axis=0,
                )
                spans[z * plane_rows : (z + 1) * plane_rows] = plane.astype(jnp.bfloat16)

        @pl.when(first << y_bits > device)
        def _():
            rows = slice(first * plane_rows, (first + far_count) * plane_rows)
            spans[rows] = jnp.zeros((far_count * plane_rows, 128), jnp.bfloat16)

    chosen_rows[...] = jnp.zeros_like(chosen_rows)

    def gate_columns(rows, branch):
        gate_rows = ready[2 * pairs, rows, :]
        return jnp.concatenate(
            [gate_rows[:, 2 * head + branch : 2 * head + branch + 1] for head in range(heads)],
            axis=0,
        )

    def span_branch(first_row, length, width):
        rows = pl.ds(first_row, length)
        scores = dot_last(
            one_sided([ready[pair, rows, :] for pair in range(pairs)], False), spans[:width]
        )
        row_place = lax.broadcasted_iota(jnp.int32, (heads * length, 1), 0) % length
        places = device * tok_rows + first_row + row_place
        has_span = places >= CMP - 1
        span_ends = lax.broadcasted_iota(jnp.int32, (1, width), 1) * CMP + CMP - 1
        scores = jnp.where(span_ends <= places, scores * score_scale, big_negative)
        peak = jnp.max(scores, axis=-1, keepdims=True)
        raw = jnp.exp(scores - peak)
        total = jnp.where(has_span, jnp.sum(raw, axis=-1, keepdims=True), 1.0)
        summed = jnp.dot(
            raw.astype(jnp.bfloat16), spans[:width], preferred_element_type=jnp.float32
        )
        summed = jnp.where(has_span, gate_columns(rows, 0) * (summed[:, 64:] / total), 0.0)
        span_log = jnp.where(has_span, peak + jnp.log(total), 0.0)
        for head in range(heads):
            piece = slice(head * length, (head + 1) * length)
            span_part[head, rows, :] = summed[piece]
            logs[0, rows, head : head + 1] = span_log[piece]

    few_spans = all_spans // 4
    few = (device + 1) * span_rows <= few_spans

    @pl.when(few)
    def _():
        for part in range(2):
            span_branch(part * (tok_rows // 2), tok_rows // 2, few_spans)

    @pl.when(jnp.logical_not(few))
    def _():
        @pl.loop(0, blocks)
        def _(block):
            span_branch(pl.multiple_of(block * block_len, block_len), block_len, all_spans)

    row_place = lax.broadcasted_iota(jnp.int32, (heads * block_len, 1), 0) % block_len
    lanes = lax.broadcasted_iota(jnp.int32, (heads * block_len, all_rows), 1)

    def chosen_branch(block, keys, values):
        rows = pl.ds(pl.multiple_of(block * block_len, block_len), block_len)
        keys[:packed] = own[0, block]
        values[:packed] = own[1, block]
        counted = jnp.int32(1)
        for number in range(named):
            source = chosen[block, number]
            start = pl.multiple_of(counted * packed, packed)
            y, slot = source & (y_count - 1), slot_of(source >> y_bits)
            keys[pl.ds(start, packed)] = arrived[y, slot, :packed, :]
            values[pl.ds(start, packed)] = arrived[y, slot, packed:block_len, :]
            counted = counted + jnp.where(source < device, 1, 0)
        queries = [ready[pairs + pair, rows, :] for pair in range(pairs)]
        half_scores = []
        blocked = jnp.where(lanes[:1] < counted * packed, 0.0, big_negative)
        for upper in (False, True):
            scores = dot_last(one_sided(queries, upper), keys[...])
            scores = scores * score_scale + blocked
            later = (lanes < packed) & (lanes + packed * upper > row_place)
            half_scores.append(jnp.where(later, big_negative, scores))
        peak = jnp.maximum(
            jnp.max(half_scores[0], axis=-1, keepdims=True),
            jnp.max(half_scores[1], axis=-1, keepdims=True),
        )
        total = 0.0
        products = []
        for upper in range(2):
            raw = jnp.exp(half_scores[upper] - peak)
            total = total + jnp.sum(raw, axis=-1, keepdims=True)
            products.append(
                jnp.dot(raw.astype(jnp.bfloat16), values[...], preferred_element_type=jnp.float32)
            )
        summed = products[0][:, :64] + products[1][:, 64:]
        scaled = gate_columns(rows, 1) * (summed / total)
        chosen_log = peak + jnp.log(total)
        pieces = []
        for head in range(heads):
            piece = slice(head * block_len, (head + 1) * block_len)
            logs[1, rows, head : head + 1] = chosen_log[piece]
            pieces.append(span_part[head, rows, :] + scaled[piece])
        for pair in range(pairs):
            both = jnp.concatenate([pieces[2 * pair], pieces[2 * pair + 1]], axis=1)
            lower, upper = both[:packed], both[packed:]
            lane_range = slice(pair * 128, (pair + 1) * 128)
            kept[block, :, lane_range] = jnp.where(core == 0, lower, upper).astype(jnp.bfloat16)
            given[block, :, lane_range] = jnp.where(core == 0, upper, lower).astype(jnp.bfloat16)

    side = chosen_rows.shape[0]

    @pl.loop(0, blocks // side)
    def _(step):
        for number in range(side):
            chosen_branch(
                step * side + number, chosen_rows.at[number, 0], chosen_rows.at[number, 1]
            )


def kernel_call(kernel, specs, operands, outputs, scratch, flops, room):
    return pl.pallas_call(
        kernel,
        out_shape=outputs,
        in_specs=[pl.BlockSpec(memory_space=space) for space in specs],
        out_specs=jax.tree.map(lambda _: pl.BlockSpec(memory_space=pltpu.VMEM), outputs),
        scratch_shapes=scratch,
        cost_estimate=pl.CostEstimate(flops=flops, bytes_accessed=4 << 20, transcendentals=0),
        compiler_params=pltpu.CompilerParams(vmem_limit_bytes=room << 20),
    )(*operands)


def turns(devices, tok_rows, head_size):
    half_size = head_size // 2
    inverse = rope_base ** (-np.arange(half_size) * 2.0 / head_size)

    def table(places):
        angles = places[:, None] * inverse[None, :]
        return jnp.asarray(np.stack([np.cos(angles), np.sin(angles)]).astype(np.float32))

    return table(np.arange(devices) * tok_rows), table(np.arange(tok_rows))


def shards(
    tokens,
    query_weight,
    key_weight,
    value_weight,
    gate_weight,
    query_gain,
    key_gain,
    out_weight,
    shared_block,
    chosen_device,
):
    tok_rows = tokens.shape[0]
    head_size = query_gain.shape[0]
    width = query_weight.shape[1]
    head_count = width // head_size
    packed = SEL // 2
    local_blocks = tok_rows // SEL
    device = lax.axis_index(KV)
    far_count, near_count, y_count = (lax.axis_size(axis) for axis in KV)
    z_count = far_count * near_count
    sent_rows = SEL + tok_rows // CMP
    starts, within = turns(z_count * y_count, tok_rows, head_size)
    bf16, f32 = jnp.bfloat16, jnp.float32
    shape = jax.ShapeDtypeStruct
    vmem, smem = pltpu.VMEM, pltpu.SMEM

    sent, own = kernel_call(
        key_kernel,
        [smem] * 2 + [vmem] * 6,
        (
            device.reshape(1),
            shared_block,
            tokens,
            key_weight.T,
            value_weight.T,
            key_gain[None],
            starts,
            within,
        ),
        (shape((sent_rows, 128), bf16), shape((2, local_blocks, packed, 128), bf16)),
        (),
        10**9,
        KEY_ROOM,
    )
    far = lax.all_gather(sent, "z_far", axis=0, tiled=True)
    column = lax.all_gather(far, "z_near", axis=0, tiled=True)
    arrived = spread(column, "y").reshape(y_count, z_count, sent_rows, 128)

    tokens_later, own, swap_weight, _ = lax.optimization_barrier(
        (tokens, own, out_weight, column)
    )
    other_weight = lax.ppermute(swap_weight, "core", [(0, 1), (1, 0)])
    ready = kernel_call(
        query_kernel,
        [smem] * 2 + [vmem] * 6,
        (
            device.reshape(1),
            lax.axis_index(TP).reshape(1),
            tokens_later,
            query_weight,
            gate_weight.T,
            jnp.concatenate([query_gain, query_gain])[None],
            starts,
            within,
        ),
        shape((2 * (width // 128) + 1, tok_rows, 128), f32),
        (),
        10**9,
        QUERY_ROOM,
    )
    ready, other_weight = lax.optimization_barrier((ready, other_weight))
    kept, given, log_weight = kernel_call(
        functools.partial(attention_kernel, far_count),
        [smem, smem, vmem, vmem, vmem],
        (
            jnp.stack([device, lax.axis_index("core")]),
            chosen_device,
            arrived,
            ready,
            own,
        ),
        (
            shape((local_blocks, packed, width), bf16),
            shape((local_blocks, packed, width), bf16),
            shape((2, tok_rows, head_count), f32),
        ),
        (
            pltpu.VMEM((4, 2, (chosen_device.shape[1] + 1) * packed, 128), bf16),
            pltpu.VMEM((y_count * z_count * (sent_rows - SEL), 128), bf16),
            pltpu.VMEM((head_count, tok_rows, head_size), f32),
        ),
        4 * 10**9,
        ATTENTION_ROOM,
    )
    taken = lax.ppermute(given, "core", [(0, 1), (1, 0)])
    own_partial = jnp.dot(
        kept.reshape(-1, width), out_weight, preferred_element_type=jnp.float32
    ).astype(bf16)
    other_partial = jnp.dot(
        taken.reshape(-1, width), other_weight, preferred_element_type=jnp.float32
    ).astype(bf16)
    pair_sum = (own_partial.astype(f32) + other_partial.astype(f32)).astype(bf16)
    pair_sum = pair_sum.reshape(local_blocks, packed, -1)
    pieces = lax.all_to_all(pair_sum, "x", split_axis=0, concat_axis=0, tiled=True)
    mixed_out = pieces.astype(f32).sum(axis=0).astype(bf16)
    return (mixed_out, log_weight)


def solution(mesh):
    torus = Mesh(mesh.devices.reshape(8, 4, 4, 4, 2), (*KV, *TP))
    return jax.shard_map(
        shards,
        mesh=torus,
        in_specs=(
            P(KV, None),
            P(None, TP),
            P(None, TP),
            P(None, TP),
            P(),
            P(),
            P(),
            P(TP, None),
            P(KV),
            P(KV, None),
        ),
        out_specs=(P((*KV, *TP), None), P(None, KV, TP)),
        check_vma=False,
    )
```
